128 devices in a mesh: sp: 32 (over z, y, core), tp: 4 (over x).
Axes of the slice: x: 4, y: 4, z: 4, core: 2. Of those that a mesh axis runs over, the one named last changes fastest.
Arguments:
- resid: bfloat16 [8192, 2048], P(('sp', 'tp')), may hold values from -0.21875 to 0.21875
- query_a: bfloat16 [8192, 1024], P('sp', 'tp'), may hold values from -6 to 6
- key_a: bfloat16 [8192, 256], P('sp', 'tp'), may hold values from -6 to 6
- value_a: bfloat16 [8192, 256], P('sp', 'tp'), may hold values from -6 to 6
- query_b: bfloat16 [8192, 1024], P('sp', 'tp'), may hold values from -6 to 6
- key_b: bfloat16 [8192, 512], P('sp', 'tp'), may hold values from -6 to 6
- value_b: bfloat16 [8192, 512], P('sp', 'tp'), may hold values from -6 to 6
- gain_qa: float32 [64], replicated, may hold values from 0.1 to 8
- gain_ka: float32 [64], replicated, may hold values from 0.1 to 8
- gain_qb: float32 [128], replicated, may hold values from 0.1 to 8
- gain_kb: float32 [128], replicated, may hold values from 0.1 to 8
- w_out_a: bfloat16 [1024, 2048], P('tp'), may hold values from -0.125 to 0.125
- w_out_b: bfloat16 [1024, 2048], P('tp'), may hold values from -0.125 to 0.125
- norm_gain: float32 [2048], replicated, may hold values from 0.1 to 1.9
- w_up: bfloat16 [2048, 8192], P('sp', 'tp'), may hold values from -0.125 to 0.125
- w_down: bfloat16 [8192, 2048], P('tp', 'sp'), may hold values from -0.0625 to 0.0625
Outputs:
- result: bfloat16 [8192, 2048], P(('sp', 'tp'))
The draws below stay inside these ranges and needn't reach their ends.
All inputs are finite; a program needn't handle non-finite values.
Results may differ from the reference program's by a relative error of at most 0.02.
The reference program's roundings to bfloat16 on the way count: a program that leaves them out, or rounds other values in their place, can miss the bound.
Values may be sent and summed in bfloat16 or wider, within the bound.
A program may use at most 128 MiB of HBM per device.

```python
import math
import jax
import jax.numpy as jnp
from jax import lax

D = 2048
FF = 8192
HD_A = 64
HD_B = 128
HEADS_A = 16
HEADS_B = 8
KV_A = 4
KV_B = 4
GRID_W = 64
TOKENS = 8192
ATT_W = 2048


def pair_draw(key, heads, kv_heads, width, salt):
    base = jax.random.fold_in(key, salt)
    keys = jnp.clip(jax.random.normal(jax.random.fold_in(base, 1), (TOKENS, kv_heads * width), jnp.float32), -6.0, 6.0)
    queries = jnp.clip(jax.random.normal(jax.random.fold_in(base, 2), (TOKENS, heads * width), jnp.float32), -6.0, 6.0)
    return (queries.astype(jnp.bfloat16), keys.astype(jnp.bfloat16))


def gain_draw(key, width, salt):
    inner = jax.random.fold_in(key, salt)
    return jnp.clip(1.0 + 0.18 * jax.random.normal(inner, (width,), jnp.float32), 0.1, 1.9)


def draw_query_a(key, part):
    return pair_draw(key, HEADS_A, KV_A, HD_A, 101)[0]


def draw_key_a(key, part):
    return pair_draw(key, HEADS_A, KV_A, HD_A, 101)[1]


def draw_query_b(key, part):
    return pair_draw(key, HEADS_B, KV_B, HD_B, 202)[0]


def draw_key_b(key, part):
    return pair_draw(key, HEADS_B, KV_B, HD_B, 202)[1]


def draw_gain_qa(key, part):
    return gain_draw(key, HD_A, 31)


def draw_gain_ka(key, part):
    return gain_draw(key, HD_A, 32)


def draw_gain_qb(key, part):
    return gain_draw(key, HD_B, 33)


def draw_gain_kb(key, part):
    return gain_draw(key, HD_B, 34)


def shard_levels(own_key, extent, pieces, least, high):
    factor_of = 1.0
    for dim, blocks in pieces:
        heights = jax.random.uniform(jax.random.fold_in(jax.random.fold_in(own_key, 6), dim), (blocks,), jnp.float32, least / len(pieces), high / len(pieces))
        factor_of = factor_of * jnp.repeat(jnp.exp(heights), extent[dim] // blocks).reshape((-1,) + (1,) * (len(extent) - 1 - dim))
    return factor_of


def normal_values(rng, extent, scale, reach, cuts=(), kind=jnp.bfloat16):
    entries = jax.random.normal(rng, extent, jnp.float32) * scale
    if len(cuts) > 0:
        entries = shard_levels(rng, extent, cuts, -0.22, 0.18) * entries
    return jnp.clip(entries, min=-reach, max=reach).astype(kind)


def setup_inputs(seed: int = 0) -> dict:
    key_of = jax.random.split(jax.random.key(seed), 17)
    return {
        "resid": normal_values(key_of[0], (TOKENS, D), 0.015, 0.21875, ((0, 128),)),
        "query_a": draw_query_a(jax.random.fold_in(key_of[16], 71), 0),
        "key_a": draw_key_a(jax.random.fold_in(key_of[16], 71), 0),
        "value_a": normal_values(key_of[3], (TOKENS, KV_A * HD_A), 1.0, 6.0, ((0, 32), (1, 4))),
        "query_b": draw_query_b(jax.random.fold_in(key_of[16], 71), 0),
        "key_b": draw_key_b(jax.random.fold_in(key_of[16], 71), 0),
        "value_b": normal_values(key_of[6], (TOKENS, KV_B * HD_B), 1.0, 6.0, ((0, 32), (1, 4))),
        "gain_qa": draw_gain_qa(jax.random.fold_in(key_of[16], 71), 0),
        "gain_ka": draw_gain_ka(jax.random.fold_in(key_of[16], 71), 0),
        "gain_qb": draw_gain_qb(jax.random.fold_in(key_of[16], 71), 0),
        "gain_kb": draw_gain_kb(jax.random.fold_in(key_of[16], 71), 0),
        "w_out_a": normal_values(key_of[11], (HEADS_A * HD_A, D), ATT_W ** -0.5, 0.125, ((0, 4),)),
        "w_out_b": normal_values(key_of[12], (HEADS_B * HD_B, D), ATT_W ** -0.5, 0.125, ((0, 4),)),
        "norm_gain": jnp.clip(1.0 + 0.18 * jax.random.normal(key_of[13], (D,), jnp.float32), 0.1, 1.9),
        "w_up": normal_values(key_of[14], (D, FF), D ** -0.5, 0.125, ((0, 32), (1, 4))),
        "w_down": normal_values(key_of[15], (FF, D), FF ** -0.5, 0.0625, ((0, 4), (1, 32))),
    }


EPS = 1e-06

def tables(count, width):
    pos = jnp.arange(count, dtype=jnp.int32)
    grid_rows = (pos // GRID_W).astype(jnp.float32)
    grid_cols = (pos % GRID_W).astype(jnp.float32)
    quarter = width // 4
    freqs = 10000.0 ** (-(2.0 * jnp.arange(quarter, dtype=jnp.float32)) / (width // 2))
    ang_r = grid_rows[:, None] * freqs
    ang_c = grid_cols[:, None] * freqs
    angles = jnp.concatenate([ang_r, ang_r, ang_c, ang_c], axis=-1)
    return (jnp.cos(angles), jnp.sin(angles))

def norm_rope(values, gain, width):
    count = values.shape[0]
    flat = values.astype(jnp.float32).reshape(count, -1, width)
    flat = flat * lax.rsqrt(lax.optimization_barrier(jnp.mean(flat * flat, axis=-1, keepdims=True)) + EPS) * gain.astype(jnp.float32)
    cosine, sine = tables(count, width)
    one, two, three, four = jnp.split(flat, 4, axis=-1)
    turned = jnp.concatenate([-two, one, -four, three], axis=-1)
    return (flat * cosine[:, None, :] + turned * sine[:, None, :]).astype(jnp.bfloat16)

def attend(queries, keys, values, width):
    count, heads = (queries.shape[0], queries.shape[1])
    kv_heads = keys.shape[1]
    groups = heads // kv_heads
    block = math.gcd(count, 256)
    keys32 = keys.astype(jnp.float32)
    vals32 = values.astype(jnp.float32).reshape(count, kv_heads, width)
    blocks = queries.reshape(count // block, block, kv_heads, groups, width)
    scale = width ** (-0.5)

    def one_block(qblock):
        scores = jnp.einsum('rkgd,pkd->kgrp', qblock.astype(jnp.float32), keys32) * scale
        top = lax.optimization_barrier(jnp.max(scores, axis=-1, keepdims=True))
        expo = jnp.exp(scores - top)
        probs = expo.astype(jnp.bfloat16).astype(jnp.float32)
        summed = jnp.einsum('kgrp,pkd->kgrd', probs, vals32)
        outputs = summed / lax.optimization_barrier(jnp.sum(expo, axis=-1))[..., None]
        return jnp.transpose(outputs, (2, 0, 1, 3)).reshape(block, heads * width).astype(jnp.bfloat16)
    return lax.map(one_block, blocks).reshape(count, heads * width)

def reference(resid, query_a, key_a, value_a, query_b, key_b, value_b, gain_qa, gain_ka, gain_qb, gain_kb, w_out_a, w_out_b, norm_gain, w_up, w_down):
    width_a = gain_qa.shape[0]
    width_b = gain_qb.shape[0]
    attn_a = attend(norm_rope(query_a, gain_qa, width_a), norm_rope(key_a, gain_ka, width_a), value_a, width_a)
    attn_b = attend(norm_rope(query_b, gain_qb, width_b), norm_rope(key_b, gain_kb, width_b), value_b, width_b)
    proj = jnp.dot(attn_a, w_out_a, preferred_element_type=jnp.float32) + jnp.dot(attn_b, w_out_b, preferred_element_type=jnp.float32)
    mid = (resid.astype(jnp.float32) + proj).astype(jnp.bfloat16)
    midf = mid.astype(jnp.float32)
    normed = (midf * lax.rsqrt(lax.optimization_barrier(jnp.mean(midf * midf, axis=-1, keepdims=True)) + EPS) * norm_gain).astype(jnp.bfloat16)
    hidden = jnp.square(jax.nn.relu(jnp.dot(normed, w_up, preferred_element_type=jnp.float32))).astype(jnp.bfloat16)
    return (midf + jnp.dot(hidden, w_down, preferred_element_type=jnp.float32)).astype(jnp.bfloat16)
```

```python
import functools
import math

import jax
import jax.numpy as jnp
import numpy as np
from jax import lax
from jax.experimental import pallas as pl
from jax.experimental.pallas import tpu as pltpu
from jax.sharding import PartitionSpec as P

MESH = pl.DeviceIdType.MESH
EPS = 1e-06
F32 = jnp.float32
BF16 = jnp.bfloat16
LOG2E = 1.4426950408889634
KV, UP, DOWN = 0, 1, 2
PLACES = (0, 3, 1, 2)


def build_tables():
    rows, cols = [], []
    for width in (64, 128):
        quarter = width // 4
        freqs = (10000.0 ** (-(2.0 * np.arange(quarter)) / (width // 2))).astype(np.float32)
        freqs = np.concatenate([freqs, freqs])
        entry = np.arange(width)
        sign = np.where((entry // quarter) % 2 == 0, -1.0, 1.0)

        def pair(count, low):
            ang = (np.arange(count, dtype=np.float32)[:, None] * freqs).astype(np.float64)
            full = np.zeros((2, count, width))
            half = slice(0, width // 2) if low else slice(width // 2, width)
            full[0][:, half] = np.cos(ang)
            full[1][:, half] = np.sin(ang)
            full[1] *= sign
            return np.tile(full, (1, 1, 128 // width)).astype(np.float32)

        rows.append(pair(128, True))
        cols.append(pair(64, False))
    row = np.concatenate(rows, axis=0)
    row = row.reshape(4, 32, 4, 128).transpose(1, 0, 2, 3).reshape(32, 16, 128)
    col = np.concatenate(cols, axis=0)
    return row, col


def nt_dot(a, b):
    return lax.dot_general(a, b, (((1,), (1,)), ((), ())), preferred_element_type=F32)


def place(k):
    return (3 * k + 3 * (k // 2) + 2 * (k // 3)) % 4


def plan():
    def wave(item):
        return [
            (item, 3, 0), (item, 1, 0), (item, 0, 3), (item, 0, 1), (item, 2, 0), (item, 0, 2),
            (item, 3, 3), (item, 3, 1), (item, 1, 3), (item, 1, 1), (item, 3, 2), (item, 1, 2),
            (item, 2, 3), (item, 2, 1), (item, 2, 2),
        ]

    k, u, d = wave(KV), wave(UP), wave(DOWN)
    steps = [[] for _ in range(16)]
    steps[1] = k[0:4]
    steps[2] = u[0:2]
    steps[3] = k[4:6]
    steps[4] = u[2:4]
    steps[5] = k[6:8]
    steps[6] = u[4:5]
    steps[7] = k[8:11]
    steps[8] = u[5:7]
    steps[9] = [k[11]]
    steps[10] = u[7:8]
    steps[11] = [k[12]]
    steps[12] = [k[13]] + u[8:9]
    steps[13] = [k[14]]
    steps[14] = u[9:11]
    steps[15] = [(DOWN, 0, 0)]
    return steps, u[11:], d


def kernel(
    qa_ref, ka_ref, va_ref, qb_ref, kb_ref, vb_ref, gains_ref, ngain_ref, rowtab_ref, coltab_ref,
    resid_hbm, woa_hbm, wob_hbm, wup_hbm, wdown_hbm,
    out_ref,
    kvbuf, wbuf, wd_in, wo, resid, qa, qb, m_a, m_b, acc_a, acc_b, attn,
    pout, rsbuf, nbuf, hidden, dbuf, frecv, stage, midbuf,
    lsem, ssem, rsem, psend, precv, xs, xr, fs, fr,
):
    sp = lax.axis_index("sp")
    x = lax.axis_index("tp")
    z, y, c = sp // 8, (sp // 2) % 4, sp % 2
    n = 1 - c
    partner = z * 8 + y * 2 + n

    def slot(da, db):
        return ((z + n * db + c * da) % 4) * 8 + ((y + n * da + c * db) % 4) * 2 + c

    def partner_slot(da, db):
        return ((z + c * db + n * da) % 4) * 8 + ((y + c * da + n * db) % 4) * 2 + n

    def event(da, db):
        return PLACES.index(da) * 4 + PLACES.index(db)

    barrier = pltpu.get_barrier_semaphore()
    others = [(slot(1, 0), x), (slot(3, 0), x), (slot(0, 1), x), (slot(0, 3), x), (partner, x)]
    others += [(sp, (x + d) % 4) for d in (1, 2, 3)]
    for dev in others:
        pl.semaphore_signal(barrier, inc=1, device_id=dev, device_id_type=MESH)

    loads = [
        pltpu.make_async_copy(wup_hbm, wbuf.at[0, sp], lsem.at[0]),
        pltpu.make_async_copy(wdown_hbm, wd_in, lsem.at[1]),
        pltpu.make_async_copy(woa_hbm, wo.at[pl.ds(0, 256)], lsem.at[2]),
        pltpu.make_async_copy(wob_hbm, wo.at[pl.ds(256, 256)], lsem.at[3]),
        pltpu.make_async_copy(resid_hbm, resid, lsem.at[4]),
    ]
    for load in loads:
        load.start()

    def region(item, index, half):
        if item == KV:
            ref, size = kvbuf.at[index], 128
        else:
            ref, size = wbuf.at[item - 1, index], 32
        if half is None:
            return ref
        return ref.at[pl.ds(half * size, size)]

    sends = []

    def send(item, ev, number, index, half, to, there):
        piece = region(item, index, half)
        copy = pltpu.make_async_remote_copy(
            src_ref=piece,
            dst_ref=piece,
            send_sem=ssem.at[item, ev, number],
            recv_sem=rsem.at[item, event(*there), 0 if half is None else half],
            device_id=(slot(*to), x),
            device_id_type=MESH,
        )
        copy.start()
        sends.append((item, ev, number, half))

    def hand_over(item, ev, index):
        piece = region(item, index, None)
        pltpu.make_async_remote_copy(
            src_ref=piece,
            dst_ref=piece,
            send_sem=psend.at[item, ev],
            recv_sem=precv.at[item, ev],
            device_id=(partner, x),
            device_id_type=MESH,
        ).start()

    def wait_in(item, ev, index, half):
        piece = region(item, index, half)
        pltpu.make_async_remote_copy(
            src_ref=piece,
            dst_ref=piece,
            send_sem=ssem.at[item, ev, 0],
            recv_sem=rsem.at[item, ev, 0 if half is None else half],
            device_id=(partner, x),
            device_id_type=MESH,
        ).wait_recv()

    def wait_partner(item, ev, index):
        piece = region(item, index, None)
        pltpu.make_async_remote_copy(
            src_ref=piece,
            dst_ref=piece,
            send_sem=psend.at[item, ev],
            recv_sem=precv.at[item, ev],
            device_id=(partner, x),
            device_id_type=MESH,
        ).wait_recv()

    def take(item, da, db):
        ev, index = event(da, db), slot(da, db)
        if da == 0 and db == 0:
            send(item, ev, 0, index, None, (1, 0), (3, 0))
            send(item, ev, 1, index, None, (3, 0), (1, 0))
            send(item, ev, 2, index, None, (0, 1), (0, 3))
            send(item, ev, 3, index, None, (0, 3), (0, 1))
        elif db == 0:
            if da == 2:
                wait_in(item, ev, index, 0)
                wait_in(item, ev, index, 1)
            else:
                wait_in(item, ev, index, None)
                if da == 3:
                    send(item, ev, 0, index, 0, (1, 0), (2, 0))
                else:
                    send(item, ev, 0, index, 1, (3, 0), (2, 0))
            send(item, ev, 2, index, None, (0, 1), (da, 3))
            send(item, ev, 3, index, None, (0, 3), (da, 1))
        elif db == 2:
            wait_in(item, ev, index, 0)
            wait_in(item, ev, index, 1)
        else:
            wait_in(item, ev, index, None)
            if db == 3:
                send(item, ev, 0, index, 0, (0, 1), (da, 2))
            else:
                send(item, ev, 0, index, 1, (0, 3), (da, 2))
        hand_over(item, ev, index)

    lane = lax.broadcasted_iota(jnp.int32, (64, 128), 1)
    low = lane < 64
    rowtab = rowtab_ref[sp]

    def rotate(v, gain, width, r):
        quarter = width // 4
        kind = 0 if width == 64 else 2
        cosine = rowtab[kind * 4 + r][None, :] + coltab_ref[kind]
        sine = rowtab[(kind + 1) * 4 + r][None, :] + coltab_ref[kind + 1]
        sq = v * v
        if width == 64:
            left = jnp.sum(jnp.where(low, sq, 0.0), axis=-1, keepdims=True)
            right = jnp.sum(jnp.where(low, 0.0, sq), axis=-1, keepdims=True)
            mean = jnp.where(low, left, right) * (1.0 / 64)
        else:
            mean = jnp.sum(sq, axis=-1, keepdims=True) * (1.0 / 128)
        u = v * lax.rsqrt(mean + EPS) * gain
        even = (lane // quarter) % 2 == 0
        turned = jnp.where(even, pltpu.roll(u, 128 - quarter, 1), pltpu.roll(u, quarter, 1))
        return u * cosine + turned * sine

    own = slot(0, 0)
    for r in range(4):
        rows = pl.ds(r * 64, 64)
        both = jnp.concatenate([ka_ref[rows, :].astype(F32), va_ref[rows, :].astype(F32)], axis=1)
        turned = rotate(both, gains_ref[1:2, :], 64, r)
        kvbuf[own, rows, 0:128] = jnp.where(low, turned, both).astype(BF16)
        kvbuf[own, rows, 128:256] = rotate(kb_ref[rows, :].astype(F32), gains_ref[3:4, :], 128, r).astype(BF16)
        kvbuf[own, rows, 256:384] = vb_ref[rows, :]

    pl.semaphore_wait(barrier, len(others))
    take(KV, 0, 0)

    for r in range(4):
        rows = pl.ds(r * 64, 64)
        for g in range(2):
            v = rotate(qa_ref[rows, g * 128 : (g + 1) * 128].astype(F32), gains_ref[0:1, :], 64, r)
            qa[pl.ds((2 * g) * 256 + r * 64, 64), :] = jnp.where(low, v, 0.0).astype(BF16)
            qa[pl.ds((2 * g + 1) * 256 + r * 64, 64), :] = jnp.where(low, pltpu.roll(v, 64, 1), 0.0).astype(BF16)
            w = rotate(qb_ref[rows, g * 128 : (g + 1) * 128].astype(F32), gains_ref[2:3, :], 128, r)
            qb[pl.ds(g * 256 + r * 64, 64), :] = w.astype(BF16)

    loads[0].wait()
    take(UP, 0, 0)

    m_a[...] = jnp.full_like(m_a, -1e30)
    m_b[...] = jnp.full_like(m_b, -1e30)
    acc_a[...] = jnp.zeros_like(acc_a)
    acc_b[...] = jnp.zeros_like(acc_b)

    loads[1].wait()
    for g in range(4):
        block = wd_in[pl.ds(g * 512, 512), :].astype(F32)
        wbuf[1, own, :, g * 512 : (g + 1) * 512] = block.T.astype(BF16)

    steps, rest_up, rest_down = plan()
    lane512 = lax.broadcasted_iota(jnp.int32, (512, 128), 1)
    scale_a = 64 ** (-0.5) * LOG2E
    scale_b = 128 ** (-0.5) * LOG2E

    def fold(queries, keys, values, m_ref, acc_ref, start, scale):
        rows = pl.ds(start, 256)
        scores = nt_dot(queries[rows, :], keys) * scale
        before = m_ref[rows, :]
        top = jnp.maximum(before, jnp.max(scores, axis=-1, keepdims=True))
        m_ref[rows, :] = top
        factor = jnp.exp2(before - top)
        expo = jnp.exp2(scores - top[:, 0:1]).astype(BF16)
        got = jnp.dot(expo, values, preferred_element_type=F32)
        if acc_ref.shape[1] == 256:
            factor = jnp.concatenate([factor, factor], axis=1)
        acc_ref[rows, :] = acc_ref[rows, :] * factor + got

    def attend(i, carry):
        for number, events in enumerate(steps):
            if events:

                @pl.when(i == number)
                def _(events=events):
                    for item, da, db in events:
                        take(item, da, db)

        da, db = place(i // 4), place(i % 4)
        mine, other = slot(da, db), partner_slot(da, db)
        wait_partner(KV, i, other)
        keys = jnp.concatenate([kvbuf[mine, :, 0:128], kvbuf[other, :, 0:128]], axis=0)
        values = jnp.where(lane512 < 64, jnp.ones_like(keys), keys)
        for h in range(4):
            fold(qa, keys, values, m_a, acc_a, h * 256, scale_a)
        keys = jnp.concatenate([kvbuf[mine, :, 128:256], kvbuf[other, :, 128:256]], axis=0)
        values = jnp.concatenate([kvbuf[mine, :, 256:384], kvbuf[other, :, 256:384]], axis=0)
        values = jnp.concatenate([values, jnp.ones_like(values)], axis=1)
        for h in range(2):
            fold(qb, keys, values, m_b, acc_b, h * 256, scale_b)
        return carry

    lax.fori_loop(0, 16, attend, 0)

    low256 = lax.broadcasted_iota(jnp.int32, (256, 128), 1) < 64
    for g in range(2):
        halves = []
        for h in (2 * g, 2 * g + 1):
            acc = acc_a[h * 256 : (h + 1) * 256, :]
            halves.append(acc / acc[:, 0:1])
        both = jnp.where(low256, pltpu.roll(halves[0], 64, 1), halves[1])
        attn[:, g * 128 : (g + 1) * 128] = both.astype(BF16)
        acc = acc_b[g * 256 : (g + 1) * 256, :]
        attn[:, 256 + g * 128 : 256 + (g + 1) * 128] = (acc[:, 0:128] / acc[:, 128:256]).astype(BF16)
    loads[2].wait()
    loads[3].wait()

    def project(j, carry):
        cols = pl.ds(pl.multiple_of(j * 512, 512), 512)
        part = jnp.dot(attn[...], wo[:, cols], preferred_element_type=F32).astype(BF16)
        for r in range(4):
            pout[r, :, cols] = part[r * 64 : (r + 1) * 64, :]
        return carry

    lax.fori_loop(0, 4, project, 0)

    def to_peer(d, src, dst, ssems, rsems):
        return pltpu.make_async_remote_copy(
            src_ref=src,
            dst_ref=dst,
            send_sem=ssems,
            recv_sem=rsems,
            device_id=(sp, (x + d) % 4),
            device_id_type=MESH,
        )

    def rs_copy(d):
        return to_peer(d, pout.at[(x + d) % 4], rsbuf.at[d - 1], xs.at[0, d - 1], xr.at[0, d - 1])

    for d in (2, 1, 3):
        rs_copy(d).start()
    for item, da, db in rest_up:
        take(item, da, db)
    for item, da, db in rest_down[0:2]:
        take(item, da, db)
    loads[4].wait()
    for d in (1, 3, 2):
        rs_copy(d).wait_recv()
    total = pout[x].astype(F32)
    for d in range(3):
        total = total + rsbuf[d].astype(F32)
    mid = (resid[...].astype(F32) + total).astype(BF16).astype(F32)
    midbuf[...] = mid
    norm = mid * lax.rsqrt(jnp.mean(mid * mid, axis=-1, keepdims=True) + EPS) * ngain_ref[...]
    nbuf[x] = norm.astype(BF16)

    def ag_copy(d, there):
        index = (x + d) % 4 if there else x
        return to_peer(d, nbuf.at[index], nbuf.at[index], xs.at[1, d - 1], xr.at[1, d - 1])

    for d in (2, 1, 3):
        ag_copy(d, False).start()
    for item, da, db in rest_down[2:6]:
        take(item, da, db)
    for ev in range(16):
        wait_partner(UP, ev, partner_slot(PLACES[ev // 4], PLACES[ev % 4]))
    for d in (1, 3, 2):
        to_peer(d, nbuf.at[(x + 4 - d) % 4], nbuf.at[(x + 4 - d) % 4], xs.at[1, d - 1], xr.at[1, d - 1]).wait_recv()

    def up(j, carry):
        cols = pl.ds(pl.multiple_of(j * 256, 256), 256)
        rows = nbuf[...].reshape(256, 2048)
        weights = wbuf[0, :, :, cols].reshape(2048, 256)
        part = jnp.maximum(jnp.dot(rows, weights, preferred_element_type=F32), 0.0)
        hidden[:, cols] = (part * part).astype(BF16)
        return carry

    lax.fori_loop(0, 8, up, 0)

    def down_copy(k, d):
        return to_peer(d, dbuf.at[(x + d) % 4, k], frecv.at[d - 1, k], fs.at[k, d - 1], fr.at[k, d - 1])

    low64 = low

    def collect(k):
        for d in (1, 3, 2):
            down_copy(k, d).wait_recv()
        total = dbuf[x, k].astype(F32)
        for d in range(3):
            total = total + frecv[d, k].astype(F32)
        for b in range(8):
            piece = total[:, (b // 2) * 128 : (b // 2) * 128 + 128]
            if b % 2 == 1:
                piece = pltpu.roll(piece, 64, 1)
            da, db = PLACES[k], PLACES[b % 4]
            stage[slot(da, db) if b < 4 else partner_slot(da, db)] = piece

    needed = {0: rest_down[6:6], 1: rest_down[6:11], 2: rest_down[11:12], 3: rest_down[12:15]}
    for k in range(4):
        for item, da, db in needed[k]:
            take(item, da, db)
        for r in range(4):
            wait_partner(DOWN, k * 4 + r, partner_slot(PLACES[k], PLACES[r]))
        blocks = [wbuf[1, slot(PLACES[k], db)] for db in PLACES]
        blocks += [wbuf[1, partner_slot(PLACES[k], db)] for db in PLACES]
        weights = jnp.concatenate(blocks, axis=0)
        part = nt_dot(hidden[...], weights).astype(BF16)
        for r in range(4):
            dbuf[r, k] = part[r * 64 : (r + 1) * 64, :]
        for d in (2, 1, 3):
            down_copy(k, d).start()
        if k > 0:
            collect(k - 1)
    collect(3)
    for pos in range(16):
        both = jnp.where(low64, stage[2 * pos], pltpu.roll(stage[2 * pos + 1], 64, 1))
        cols = slice(pos * 128, pos * 128 + 128)
        out_ref[:, cols] = (midbuf[:, cols] + both).astype(BF16)

    for item, ev, number, half in sends:
        index = slot(PLACES[ev // 4], PLACES[ev % 4])
        piece = region(item, index, half)
        pltpu.make_async_remote_copy(
            src_ref=piece, dst_ref=piece, send_sem=ssem.at[item, ev, number], recv_sem=rsem.at[item, ev, 0],
            device_id=(partner, x), device_id_type=MESH,
        ).wait_send()
    for item in (KV, UP, DOWN):
        for ev in range(16):
            piece = region(item, slot(PLACES[ev // 4], PLACES[ev % 4]), None)
            pltpu.make_async_remote_copy(
                src_ref=piece, dst_ref=piece, send_sem=psend.at[item, ev], recv_sem=precv.at[item, ev],
                device_id=(partner, x), device_id_type=MESH,
            ).wait_send()
    for d in (1, 2, 3):
        rs_copy(d).wait_send()
        ag_copy(d, False).wait_send()
        for k in range(4):
            down_copy(k, d).wait_send()


def local(
    resid, query_a, key_a, value_a, query_b, key_b, value_b, gain_qa, gain_ka, gain_qb, gain_kb,
    w_out_a, w_out_b, norm_gain, w_up, w_down,
):
    rowtab, coltab = build_tables()
    gains = jnp.stack([jnp.tile(gain_qa, 2), jnp.tile(gain_ka, 2), gain_qb, gain_kb])
    vmem = pl.BlockSpec(memory_space=pltpu.VMEM)
    anywhere = pl.BlockSpec(memory_space=pl.ANY)
    dma = pltpu.SemaphoreType.DMA
    return pl.pallas_call(
        kernel,
        out_shape=jax.ShapeDtypeStruct((64, 2048), BF16),
        in_specs=[vmem] * 10 + [anywhere] * 5,
        out_specs=vmem,
        scratch_shapes=[
            pltpu.VMEM((32, 256, 384), BF16),
            pltpu.VMEM((2, 32, 64, 2048), BF16),
            pltpu.VMEM((2048, 64), BF16),
            pltpu.VMEM((512, 2048), BF16),
            pltpu.VMEM((64, 2048), BF16),
            pltpu.VMEM((1024, 128), BF16),
            pltpu.VMEM((512, 128), BF16),
            pltpu.VMEM((1024, 128), F32),
            pltpu.VMEM((512, 128), F32),
            pltpu.VMEM((1024, 128), F32),
            pltpu.VMEM((512, 256), F32),
            pltpu.VMEM((256, 512), BF16),
            pltpu.VMEM((4, 64, 2048), BF16),
            pltpu.VMEM((3, 64, 2048), BF16),
            pltpu.VMEM((4, 64, 2048), BF16),
            pltpu.VMEM((256, 2048), BF16),
            pltpu.VMEM((4, 4, 64, 512), BF16),
            pltpu.VMEM((3, 4, 64, 512), BF16),
            pltpu.VMEM((32, 64, 128), F32),
            pltpu.VMEM((64, 2048), F32),
            dma((5,)),
            dma((3, 16, 4)),
            dma((3, 16, 2)),
            dma((3, 16)),
            dma((3, 16)),
            dma((2, 3)),
            dma((2, 3)),
            dma((4, 3)),
            dma((4, 3)),
        ],
        compiler_params=pltpu.CompilerParams(
            collective_id=0, has_side_effects=True, vmem_limit_bytes=58 * 1024 * 1024
        ),
    )(
        query_a, key_a, value_a, query_b, key_b, value_b, gains, norm_gain.reshape(1, -1),
        jnp.asarray(rowtab), jnp.asarray(coltab),
        resid, w_out_a, w_out_b, w_up, w_down,
    )


def solution(mesh):
    return jax.shard_map(
        local,
        mesh=mesh,
        in_specs=(
            P(("sp", "tp"), None),
            P("sp", "tp"),
            P("sp", "tp"),
            P("sp", "tp"),
            P("sp", "tp"),
            P("sp", "tp"),
            P("sp", "tp"),
            P(),
            P(),
            P(),
            P(),
            P("tp", None),
            P("tp", None),
            P(),
            P("sp", "tp"),
            P("tp", "sp"),
        ),
        out_specs=P(("sp", "tp"), None),
        check_vma=False,
    )
```

```python
import functools
import math

import jax
import jax.numpy as jnp
import numpy as np
from jax import lax
from jax.experimental import pallas as pl
from jax.experimental.pallas import tpu as pltpu
from jax.sharding import PartitionSpec as P

MESH = pl.DeviceIdType.MESH
EPS = 1e-06
F32 = jnp.float32
BF16 = jnp.bfloat16
LOG2E = 1.4426950408889634
KV, UP, DOWN = 0, 1, 2
ORDER = (
    (0, 0), (3, 0), (1, 0), (0, 3), (0, 1), (2, 0), (3, 3), (3, 1),
    (1, 3), (1, 1), (0, 2), (2, 3), (2, 1), (3, 2), (1, 2), (2, 2),
)


def build_tables():
    rows, cols = [], []
    for width in (64, 128):
        quarter = width // 4
        freqs = (10000.0 ** (-(2.0 * np.arange(quarter)) / (width // 2))).astype(np.float32)
        freqs = np.concatenate([freqs, freqs])
        entry = np.arange(width)
        sign = np.where((entry // quarter) % 2 == 0, -1.0, 1.0)

        def pair(count, low):
            ang = (np.arange(count, dtype=np.float32)[:, None] * freqs).astype(np.float64)
            full = np.zeros((2, count, width))
            half = slice(0, width // 2) if low else slice(width // 2, width)
            full[0][:, half] = np.cos(ang)
            full[1][:, half] = np.sin(ang)
            full[1] *= sign
            return np.tile(full, (1, 1, 128 // width)).astype(np.float32)

        rows.append(pair(128, True))
        cols.append(pair(64, False))
    row = np.concatenate(rows, axis=0)
    row = row.reshape(4, 32, 4, 128).transpose(1, 0, 2, 3).reshape(32, 16, 128)
    col = np.concatenate(cols, axis=0)
    return row, col


def nt_dot(a, b):
    return lax.dot_general(a, b, (((1,), (1,)), ((), ())), preferred_element_type=F32)


def nn_dot(a, b):
    return jnp.dot(a, b, preferred_element_type=F32)


def pick(i, values):
    result = jnp.int32(values[0])
    for number, value in enumerate(values[1:]):
        result = jnp.where(i == number + 1, jnp.int32(value), result)
    return result


PLAN = {
    1: [(0, 1), (0, 2)],
    2: [(0, 3)],
    3: [(0, 4)],
    4: [(0, 5)],
    5: [(0, 6)],
    6: [(0, 7)],
    7: [(0, 8)],
    8: [(0, 9), (1, "b")],
    9: [(0, 10)],
    10: [(0, 11)],
    11: [(0, 12), (1, 1), (1, 2)],
    12: [(0, 13)],
    13: [(0, 14)],
    14: [(1, 5), (1, 3), (1, 4), (0, 15)],
    15: [],
    16: [],
}
AFTER_PROJECT = [(1, 6), (2, "b"), (1, 7), (2, "a"), "combine", (1, 8), (1, 9), (1, 11), (1, 12), (2, 1), (2, 2), (1, 10)]
AFTER_SUM = [(2, 5), (2, 4), (1, 13), "relay", (2, 3), (1, 14), (1, 15), (2, 6), (2, 7)]
AMID_UP = [(2, 8), (2, 9)]
BEFORE_DOWN = {0: [], 1: [(2, 11), (2, 12)], 2: [(2, 10)], 3: [(2, 13), (2, 14), (2, 15)]}


def kernel(
    qa_ref, ka_ref, va_ref, qb_ref, kb_ref, vb_ref, gqa_ref, gka_ref, gqb_ref, gkb_ref,
    ngain_ref, rowtab_ref, coltab_ref,
    resid_hbm, woa_hbm, wob_hbm, wup_hbm, wdown_hbm,
    out_ref,
    kvbuf, wbuf, wo, resid, qa, qb, s_even, s_odd, tops, acc_a, acc_b, attn,
    pout, phalf, rsbuf, nbuf, hidden, dbuf, dhalf, frecv, stage, midbuf,
    lsem, ssem, rsem, psend, precv, xs, xr, gs, gr,
):
    sp = lax.axis_index("sp")
    x = lax.axis_index("tp")
    z, y, c = sp // 8, (sp // 2) % 4, sp % 2
    n = 1 - c
    partner = z * 8 + y * 2 + n

    def slot(da, db):
        return ((z + n * db + c * da) % 4) * 8 + ((y + n * da + c * db) % 4) * 2 + c

    def partner_slot(da, db):
        return ((z + c * db + n * da) % 4) * 8 + ((y + c * da + n * db) % 4) * 2 + n

    def event(da, db):
        return ORDER.index((da, db))

    barrier = pltpu.get_barrier_semaphore()
    others = [(slot(1, 0), x), (slot(3, 0), x), (slot(0, 1), x), (slot(0, 3), x), (partner, x)]
    others += [(sp, (x + d) % 4) for d in (1, 3)]
    for dev in others:
        pl.semaphore_signal(barrier, inc=1, device_id=dev, device_id_type=MESH)

    loads = [
        pltpu.make_async_copy(wup_hbm, wbuf.at[0, sp], lsem.at[0]),
        pltpu.make_async_copy(wdown_hbm, wbuf.at[1, sp], lsem.at[1]),
        pltpu.make_async_copy(woa_hbm, wo.at[pl.ds(0, 256)], lsem.at[2]),
        pltpu.make_async_copy(wob_hbm, wo.at[pl.ds(256, 256)], lsem.at[3]),
        pltpu.make_async_copy(resid_hbm, resid, lsem.at[4]),
    ]
    for load in loads:
        load.start()

    def region(item, index, half):
        if item == KV:
            ref, size = kvbuf.at[index], 384
        else:
            ref, size = wbuf.at[item - 1, index], 32
        if half is None:
            return ref
        return ref.at[pl.ds(half * size, size)]

    sends = []

    def send(item, ev, number, index, half, to, there):
        piece = region(item, index, half)
        copy = pltpu.make_async_remote_copy(
            src_ref=piece,
            dst_ref=piece,
            send_sem=ssem.at[item, ev, number],
            recv_sem=rsem.at[item, event(*there), 0 if half is None else half],
            device_id=(slot(*to), x),
            device_id_type=MESH,
        )
        copy.start()
        sends.append((item, ev, number, half))

    def hand_over(item, ev, index):
        piece = region(item, index, None)
        pltpu.make_async_remote_copy(
            src_ref=piece,
            dst_ref=piece,
            send_sem=psend.at[item, ev],
            recv_sem=precv.at[item, ev],
            device_id=(partner, x),
            device_id_type=MESH,
        ).start()

    def wait_in(item, ev, index, half):
        piece = region(item, index, half)
        pltpu.make_async_remote_copy(
            src_ref=piece,
            dst_ref=piece,
            send_sem=ssem.at[item, ev, 0],
            recv_sem=rsem.at[item, ev, 0 if half is None else half],
            device_id=(partner, x),
            device_id_type=MESH,
        ).wait_recv()

    def wait_partner(item, ev, index):
        piece = region(item, index, None)
        pltpu.make_async_remote_copy(
            src_ref=piece,
            dst_ref=piece,
            send_sem=psend.at[item, ev],
            recv_sem=precv.at[item, ev],
            device_id=(partner, x),
            device_id_type=MESH,
        ).wait_recv()

    def take(item, number):
        with jax.named_scope(f"take{item}_{number}"):
            if number in ("a", "b"):
                start_own(item, number)
            else:
                take_in(item, *ORDER[number])

    def start_own(item, ring):
        index = slot(0, 0)
        if ring == "a":
            send(item, 0, 0, index, None, (1, 0), (3, 0))
            send(item, 0, 1, index, None, (3, 0), (1, 0))
        else:
            send(item, 0, 2, index, None, (0, 1), (0, 3))
            send(item, 0, 3, index, None, (0, 3), (0, 1))
            hand_over(item, 0, index)

    def take_in(item, da, db):
        ev, index = event(da, db), slot(da, db)
        if da == 0 and db == 0:
            raise ValueError(item)
        elif db == 0:
            if da == 2:
                wait_in(item, ev, index, 0)
                wait_in(item, ev, index, 1)
            else:
                wait_in(item, ev, index, None)
                if da == 3:
                    send(item, ev, 0, index, 0, (1, 0), (2, 0))
                else:
                    send(item, ev, 0, index, 1, (3, 0), (2, 0))
            send(item, ev, 2, index, None, (0, 1), (da, 3))
            send(item, ev, 3, index, None, (0, 3), (da, 1))
        elif db == 2:
            wait_in(item, ev, index, 0)
            wait_in(item, ev, index, 1)
        else:
            wait_in(item, ev, index, None)
            if db == 3:
                send(item, ev, 0, index, 0, (0, 1), (da, 2))
            else:
                send(item, ev, 0, index, 1, (0, 3), (da, 2))
        hand_over(item, ev, index)

    lane = lax.broadcasted_iota(jnp.int32, (64, 128), 1)
    low = lane < 64
    rowtab = rowtab_ref[sp]

    def both_heads(ref):
        return jnp.concatenate([ref[...], ref[...]], axis=1)

    def rotate(v, gain, width, r, s):
        quarter = width // 4
        kind = 0 if width == 64 else 2

        def angles(which):
            across = rowtab[which * 4 + r : which * 4 + r + 1]
            if s != r:
                across = jnp.where(low[0:1], across, rowtab[which * 4 + s : which * 4 + s + 1])
            return across + coltab_ref[which]

        sq = v * v
        if width == 64:
            left = jnp.sum(jnp.where(low, sq, 0.0), axis=-1, keepdims=True)
            right = jnp.sum(jnp.where(low, 0.0, sq), axis=-1, keepdims=True)
            mean = jnp.where(low, left, right) * (1.0 / 64)
        else:
            mean = jnp.sum(sq, axis=-1, keepdims=True) * (1.0 / 128)
        u = v * lax.rsqrt(mean + EPS) * gain
        even = (lane // quarter) % 2 == 0
        turned = jnp.where(even, pltpu.roll(u, 128 - quarter, 1), pltpu.roll(u, quarter, 1))
        return u * angles(kind) + turned * angles(kind + 1)

    own = slot(0, 0)
    turned = ka_ref[...].astype(F32)
    turned = jnp.concatenate([turned[:, 0:128], turned[:, 128:256]], axis=0).T
    gain = both_heads(gka_ref)
    for r in range(2):
        block = rotate(turned[r * 64 : (r + 1) * 64], gain, 64, r, r + 2)
        kvbuf[own, r * 64 : (r + 1) * 64, :] = block.astype(BF16)
    for r in range(4):
        block = rotate(kb_ref[r * 64 : (r + 1) * 64, :].astype(F32), gkb_ref[...], 128, r, r)
        kvbuf[own, 128 + r * 64 : 192 + r * 64, :] = block.astype(BF16)
    for half in range(2):
        tokens = slice(half * 128, half * 128 + 128)
        kvbuf[own, 384 + half * 64 : 448 + half * 64, :] = va_ref[:, tokens]
        kvbuf[own, 512 + half * 128 : 640 + half * 128, :] = vb_ref[tokens, :].astype(F32).T.astype(BF16)

    with jax.named_scope("barrier"):
        pl.semaphore_wait(barrier, len(others))
    take(KV, "a")
    take(KV, "b")
    loads[0].wait()
    take(UP, "a")

    with jax.named_scope("queries"):
        gain_a = both_heads(gqa_ref)
        for g in range(2):
            lanes = slice(g * 128, g * 128 + 128)
            rows = [slice(r * 64, r * 64 + 64) for r in range(4)]
            heads = [rotate(qa_ref[rows[r], lanes].astype(F32), gain_a, 64, r, r) for r in range(4)]
            heads = jnp.concatenate(heads, axis=0).T.astype(BF16)
            for h in range(2):
                head = heads[h * 64 : h * 64 + 64]
                qa[2 * g + h, 0:64, 0:256] = head
                qa[2 * g + h, 0:64, 256:512] = jnp.zeros_like(head)
                qa[2 * g + h, 64:128, 0:256] = jnp.zeros_like(head)
                qa[2 * g + h, 64:128, 256:512] = head
            heads = [rotate(qb_ref[rows[r], lanes].astype(F32), gqb_ref[...], 128, r, r) for r in range(4)]
            qb[g] = jnp.concatenate(heads, axis=0).T.astype(BF16)
        tops[...] = jnp.full_like(tops, -1e30)
        acc_a[...] = jnp.zeros_like(acc_a)
        acc_b[...] = jnp.zeros_like(acc_b)

    scale_a = 64 ** (-0.5) * LOG2E
    scale_b = 128 ** (-0.5) * LOG2E

    def turned_values(pieces):
        values = jnp.concatenate(pieces, axis=1)
        return jnp.concatenate([values, jnp.ones((16, 512), BF16)], axis=0)

    def score(pair, target):
        keys_a = jnp.concatenate([kvbuf[s, 0:128, :] for s in pair], axis=0)
        keys_b = jnp.concatenate([kvbuf[s, 128:384, :] for s in pair], axis=0)

        def one(h):
            if h < 4:
                scores = nn_dot(keys_a, qa[h]) * scale_a
                scores = jnp.concatenate([scores[:, 0:256], scores[:, 256:512]], axis=0)
            else:
                scores = nn_dot(keys_b, qb[h - 4]) * scale_b
            target[h] = scores
            before = tops[h, 0:1, :]
            top = jnp.maximum(before, jnp.max(scores, axis=0, keepdims=True))
            tops[h, 0:1, :] = top
            tops[h, 1:2, :] = jnp.exp2(before - top)

        return one

    def gather_values(pair):
        def one(h):
            if h < 4:
                return turned_values([kvbuf[s, 384 + 64 * half : 448 + 64 * half, :] for half in range(2) for s in pair])
            return turned_values([kvbuf[s, 512 + 128 * half : 640 + 128 * half, :] for s in pair for half in range(2)])

        return one(0), one(4)

    def use(source, h, values, top, factor):
        expo = jnp.exp2(source[h] - top).astype(BF16)
        got = nn_dot(values[0] if h < 4 else values[1], expo)
        acc, index = (acc_a, h) if h < 4 else (acc_b, h - 4)
        acc[index] = acc[index] * factor + got

    def both(now, after, source, target):
        values = gather_values(now)
        scorer = None if after is None else score(after, target)
        for h in range(6):
            top, factor = tops[h, 0:1, :], tops[h, 1:2, :]
            if scorer is not None:
                scorer(h)
            use(source, h, values, top, factor)

    def my_block(t, shift):
        places = ORDER[shift::2]
        return slot(pick(t, [p[0] for p in places]), pick(t, [p[1] for p in places]))

    def partner_block(t, shift):
        places = ORDER[shift::2]
        return partner_slot(pick(t, [p[0] for p in places]), pick(t, [p[1] for p in places]))

    def ready(t, shift):
        for number in range(6):
            if PLAN.get(2 * number + shift):

                @pl.when(t == number)
                def _(number=number):
                    for what in PLAN[2 * number + shift]:
                        take(*what)

    def fetch(number, t, shift):
        theirs = partner_block(t, shift - 1)
        with jax.named_scope("pwait"):
            wait_partner(KV, number - 1, theirs)
        return my_block(t, shift + 1), theirs

    def attend(t, pair):
        with jax.named_scope("step"):
            ready(t, 2)
            middle = fetch(2 * t + 2, t, 2)
            both(pair, middle, s_odd, s_even)
            ready(t, 3)
            after = fetch(2 * t + 3, t, 3)
            both(middle, after, s_even, s_odd)
        return after

    loads[1].wait()
    with jax.named_scope("first"):
        wait_partner(KV, 0, partner)
        pair = (own, partner)
        first = score(pair, s_even)
        for h in range(6):
            first(h)
        for what in PLAN[1]:
            take(*what)
        after = (slot(*ORDER[1]), slot(*ORDER[2]))
        both(pair, after, s_even, s_odd)
    pair = lax.fori_loop(0, 6, attend, after)
    with jax.named_scope("laststep"):
        for what in PLAN[14]:
            take(*what)
        theirs = partner_slot(*ORDER[13])
        wait_partner(KV, 13, theirs)
        middle = (slot(*ORDER[15]), theirs)
        both(pair, middle, s_odd, s_even)
        for what in PLAN[15]:
            take(*what)
        after = (partner_slot(*ORDER[14]), partner_slot(*ORDER[15]))
        wait_partner(KV, 14, after[0])
        wait_partner(KV, 15, after[1])
        both(middle, after, s_even, s_odd)
        both(after, None, s_odd, None)
        for what in PLAN[16]:
            take(*what)

    for h in range(4):
        acc = acc_a[h]
        acc_a[h, 0:64, :] = acc[0:64] / acc[64:65]
    for g in range(2):
        both_rows = jnp.concatenate([acc_a[2 * g, 0:64, :], acc_a[2 * g + 1, 0:64, :]], axis=0)
        attn[:, g * 128 : (g + 1) * 128] = both_rows.T.astype(BF16)
        acc = acc_b[g]
        attn[:, 256 + g * 128 : 256 + (g + 1) * 128] = (acc[0:128] / acc[128:129]).T.astype(BF16)
    loads[2].wait()
    loads[3].wait()

    def project(j, carry):
        cols = pl.ds(pl.multiple_of(j * 512, 512), 512)
        part = jnp.dot(attn[...], wo[:, cols], preferred_element_type=F32).astype(BF16)
        for r in range(4):
            pout[r, :, cols] = part[r * 64 : (r + 1) * 64, :]
        return carry

    with jax.named_scope("project"):
        lax.fori_loop(0, 4, project, 0)

    def to_peer(forward, src, dst, send_sem, recv_sem):
        return pltpu.make_async_remote_copy(
            src_ref=src,
            dst_ref=dst,
            send_sem=send_sem,
            recv_sem=recv_sem,
            device_id=(sp, (x + (1 if forward else 3)) % 4),
            device_id_type=MESH,
        )

    class TpSum:
        def __init__(self, number, blocks, halves, received):
            self.number, self.blocks, self.halves, self.received = number, blocks, halves, received
            width = received(0).shape[1] // 2
            self.parts = (pl.ds(0, width), pl.ds(width, width))

        def copy(self, kind, way):
            near = self.blocks((x + (1, 3)[way]) % 4)
            if kind == 0:
                src, dst = self.blocks((x + 2) % 4).at[:, self.parts[way]], self.halves(way)
            else:
                part = self.parts[1 - way] if kind == 1 else self.parts[way]
                src, dst = near.at[:, part], self.received(way).at[:, part]
            return to_peer(way == 0, src, dst, xs.at[self.number, kind, way], xr.at[self.number, kind, way])

        def start(self):
            for kind in (0, 1):
                for way in (0, 1):
                    self.copy(kind, way).start()

        def combine(self):
            for way in (0, 1):
                self.copy(0, way).wait_recv()
                near, part = self.blocks((x + (1, 3)[way]) % 4), self.parts[way]
                near[:, part] = (near[:, part].astype(F32) + self.halves(way)[...].astype(F32)).astype(BF16)
                self.copy(2, way).start()

        def total(self):
            for kind in (1, 2):
                for way in (0, 1):
                    self.copy(kind, way).wait_recv()
            return self.blocks(x)[...].astype(F32) + self.received(0)[...].astype(F32) + self.received(1)[...].astype(F32)

        def drain(self):
            for kind in (0, 1, 2):
                for way in (0, 1):
                    self.copy(kind, way).wait_send()

    proj = TpSum(0, lambda r: pout.at[r], lambda w: phalf.at[w], lambda w: rsbuf.at[w])
    proj.start()
    for what in AFTER_PROJECT:
        if what == "combine":
            with jax.named_scope("combine"):
                proj.combine()
        else:
            take(*what)
    loads[4].wait()
    with jax.named_scope("rswait"):
        total = proj.total()
    mid = (resid[...].astype(F32) + total).astype(BF16).astype(F32)
    midbuf[...] = mid
    norm = mid * lax.rsqrt(jnp.mean(mid * mid, axis=-1, keepdims=True) + EPS) * ngain_ref[...]
    nbuf[x] = norm.astype(BF16)

    halves = (pl.ds(0, 1024), pl.ds(1024, 1024))

    def rows_copy(kind, way, arriving):
        hops = (1 if kind < 2 else 2) if arriving else (0 if kind < 2 else 1)
        block = (x + 4 - hops) % 4 if way == 0 else (x + hops) % 4
        part = halves[1 - way] if kind == 1 else halves[way]
        piece = nbuf.at[block, :, part]
        return to_peer(way == 0, piece, piece, gs.at[kind, way], gr.at[kind, way])

    for kind in (0, 1):
        for way in (0, 1):
            rows_copy(kind, way, False).start()
    for what in AFTER_SUM:
        if what == "relay":
            with jax.named_scope("relay"):
                for way in (0, 1):
                    rows_copy(0, way, True).wait_recv()
                    rows_copy(2, way, False).start()
        else:
            take(*what)
    with jax.named_scope("upwait"):
        for ev in range(16):
            wait_partner(UP, ev, partner_slot(*ORDER[ev]))
    with jax.named_scope("rowswait"):
        for kind in (1, 2):
            for way in (0, 1):
                rows_copy(kind, way, True).wait_recv()

    def up(j, carry):
        cols = pl.ds(pl.multiple_of(j * 256, 256), 256)
        rows = nbuf[...].reshape(256, 2048)
        weights = wbuf[0, :, :, cols].reshape(2048, 256)
        part = jnp.maximum(jnp.dot(rows, weights, preferred_element_type=F32), 0.0)
        hidden[:, cols] = (part * part).astype(BF16)
        return carry

    with jax.named_scope("up"):
        lax.fori_loop(0, 4, up, 0)
    for what in AMID_UP:
        take(*what)
    with jax.named_scope("up"):
        lax.fori_loop(4, 8, up, 0)

    sums = [
        TpSum(k + 1, lambda r, k=k: dbuf.at[r, k], lambda w, k=k: dhalf.at[k, w], lambda w, k=k: frecv.at[k, w])
        for k in range(4)
    ]

    low64 = low

    def collect(k):
        total = sums[k].total()
        for b in range(8):
            piece = total[:, (b // 2) * 128 : (b // 2) * 128 + 128]
            if b % 2 == 1:
                piece = pltpu.roll(piece, 64, 1)
            place = ORDER[4 * k + b % 4]
            stage[slot(*place) if b < 4 else partner_slot(*place)] = piece

    for k in range(4):
        for what in BEFORE_DOWN[k]:
            take(*what)
        places = ORDER[4 * k : 4 * k + 4]
        for r in range(4):
            wait_partner(DOWN, k * 4 + r, partner_slot(*places[r]))
        blocks = [wbuf[1, slot(*place)] for place in places]
        blocks += [wbuf[1, partner_slot(*place)] for place in places]
        weights = jnp.concatenate(blocks, axis=0)
        with jax.named_scope(f"down{k}"):
            part = nt_dot(hidden[...], weights).astype(BF16)
            for r in range(4):
                dbuf[r, k] = part[r * 64 : (r + 1) * 64, :]
        sums[k].start()
        if k > 0:
            with jax.named_scope(f"combine{k - 1}"):
                sums[k - 1].combine()
        if k > 1:
            with jax.named_scope(f"collect{k - 2}"):
                collect(k - 2)
    with jax.named_scope("combine3"):
        sums[3].combine()
    with jax.named_scope("collect23"):
        collect(2)
        collect(3)
    for pos in range(16):
        both = jnp.where(low64, stage[2 * pos], pltpu.roll(stage[2 * pos + 1], 64, 1))
        cols = slice(pos * 128, pos * 128 + 128)
        out_ref[:, cols] = (midbuf[:, cols] + both).astype(BF16)

    for item, ev, number, half in sends:
        index = slot(*ORDER[ev])
        piece = region(item, index, half)
        pltpu.make_async_remote_copy(
            src_ref=piece, dst_ref=piece, send_sem=ssem.at[item, ev, number], recv_sem=rsem.at[item, ev, 0],
            device_id=(partner, x), device_id_type=MESH,
        ).wait_send()
    for item in (KV, UP, DOWN):
        for ev in range(16):
            piece = region(item, slot(*ORDER[ev]), None)
            pltpu.make_async_remote_copy(
                src_ref=piece, dst_ref=piece, send_sem=psend.at[item, ev], recv_sem=precv.at[item, ev],
                device_id=(partner, x), device_id_type=MESH,
            ).wait_send()
    for sum_over in [proj] + sums:
        sum_over.drain()
    for kind in (0, 1, 2):
        for way in (0, 1):
            rows_copy(kind, way, False).wait_send()


def local(
    resid, query_a, key_a, value_a, query_b, key_b, value_b, gain_qa, gain_ka, gain_qb, gain_kb,
    w_out_a, w_out_b, norm_gain, w_up, w_down,
):
    rowtab, coltab = build_tables()
    vmem = pl.BlockSpec(memory_space=pltpu.VMEM)
    anywhere = pl.BlockSpec(memory_space=pl.ANY)
    dma = pltpu.SemaphoreType.DMA
    return pl.pallas_call(
        kernel,
        out_shape=jax.ShapeDtypeStruct((64, 2048), BF16),
        in_specs=[vmem] * 13 + [anywhere] * 5,
        out_specs=vmem,
        scratch_shapes=[
            pltpu.VMEM((32, 768, 128), BF16),
            pltpu.VMEM((2, 32, 64, 2048), BF16),
            pltpu.VMEM((512, 2048), BF16),
            pltpu.VMEM((64, 2048), BF16),
            pltpu.VMEM((4, 128, 512), BF16),
            pltpu.VMEM((2, 128, 256), BF16),
            pltpu.VMEM((6, 512, 256), F32),
            pltpu.VMEM((6, 512, 256), F32),
            pltpu.VMEM((6, 8, 256), F32),
            pltpu.VMEM((4, 80, 256), F32),
            pltpu.VMEM((2, 144, 256), F32),
            pltpu.VMEM((256, 512), BF16),
            pltpu.VMEM((4, 64, 2048), BF16),
            pltpu.VMEM((2, 64, 1024), BF16),
            pltpu.VMEM((2, 64, 2048), BF16),
            pltpu.VMEM((4, 64, 2048), BF16),
            pltpu.VMEM((256, 2048), BF16),
            pltpu.VMEM((4, 4, 64, 512), BF16),
            pltpu.VMEM((4, 2, 64, 256), BF16),
            pltpu.VMEM((4, 2, 64, 512), BF16),
            pltpu.VMEM((32, 64, 128), F32),
            pltpu.VMEM((64, 2048), F32),
            dma((5,)),
            dma((3, 16, 4)),
            dma((3, 16, 2)),
            dma((3, 16)),
            dma((3, 16)),
            dma((5, 3, 2)),
            dma((5, 3, 2)),
            dma((3, 2)),
            dma((3, 2)),
        ],
        compiler_params=pltpu.CompilerParams(
            collective_id=0, has_side_effects=True, vmem_limit_bytes=58 * 1024 * 1024
        ),
    )(
        query_a, key_a.T, value_a.T, query_b, key_b, value_b,
        gain_qa.reshape(1, -1), gain_ka.reshape(1, -1), gain_qb.reshape(1, -1), gain_kb.reshape(1, -1),
        norm_gain.reshape(1, -1), jnp.asarray(rowtab), jnp.asarray(coltab),
        resid, w_out_a, w_out_b, w_up, w_down.T,
    )


def solution(mesh):
    return jax.shard_map(
        local,
        mesh=mesh,
        in_specs=(
            P(("sp", "tp"), None),
            P("sp", "tp"),
            P("sp", "tp"),
            P("sp", "tp"),
            P("sp", "tp"),
            P("sp", "tp"),
            P("sp", "tp"),
            P(),
            P(),
            P(),
            P(),
            P("tp", None),
            P("tp", None),
            P(),
            P("sp", "tp"),
            P("tp", "sp"),
        ),
        out_specs=P(("sp", "tp"), None),
        check_vma=False,
    )
```

```python
import functools
import math

import jax
import jax.numpy as jnp
import numpy as np
from jax import lax
from jax.experimental import pallas as pl
from jax.experimental.pallas import tpu as pltpu
from jax.sharding import PartitionSpec as P

MESH = pl.DeviceIdType.MESH
EPS = 1e-06
F32 = jnp.float32
BF16 = jnp.bfloat16
LOG2E = 1.4426950408889634
KV, UP, DOWN = 0, 1, 2
ORDER = (
    (0, 0), (3, 0), (1, 0), (0, 3), (0, 1), (2, 0), (3, 3), (3, 1),
    (1, 3), (1, 1), (0, 2), (2, 3), (2, 1), (3, 2), (1, 2), (2, 2),
)


def build_tables():
    rows, cols = [], []
    for width in (64, 128):
        quarter = width // 4
        freqs = (10000.0 ** (-(2.0 * np.arange(quarter)) / (width // 2))).astype(np.float32)
        freqs = np.concatenate([freqs, freqs])
        entry = np.arange(width)
        sign = np.where((entry // quarter) % 2 == 0, -1.0, 1.0)

        def pair(count, low):
            ang = (np.arange(count, dtype=np.float32)[:, None] * freqs).astype(np.float64)
            full = np.zeros((2, count, width))
            half = slice(0, width // 2) if low else slice(width // 2, width)
            full[0][:, half] = np.cos(ang)
            full[1][:, half] = np.sin(ang)
            full[1] *= sign
            return np.tile(full, (1, 1, 128 // width)).astype(np.float32)

        rows.append(pair(128, True))
        cols.append(pair(64, False))
    row = np.concatenate(rows, axis=0)
    row = row.reshape(4, 32, 4, 128).transpose(1, 0, 2, 3).reshape(32, 16, 128)
    col = np.concatenate(cols, axis=0)
    return row, col


def nt_dot(a, b):
    return lax.dot_general(a, b, (((1,), (1,)), ((), ())), preferred_element_type=F32)


def nn_dot(a, b):
    return jnp.dot(a, b, preferred_element_type=F32)


def pick(i, values):
    result = jnp.int32(values[0])
    for number, value in enumerate(values[1:]):
        result = jnp.where(i == number + 1, jnp.int32(value), result)
    return result


PLAN = {
    1: [(0, 1), (0, 2), (0, 3), (0, 4)],
    4: [(0, 5)],
    5: [(0, 6), (0, 7)],
    7: [(0, 8), (0, 9)],
    8: [(0, 10)],
    10: [(0, 11), (0, 12)],
    11: [(0, 13), (1, "b")],
    12: [(0, 14)],
    14: [(0, 15), (1, 1), (1, 2)],
    15: [],
    16: [(1, 3), (1, 4)],
}
AFTER_PROJECT = [(1, 5), (1, 6), (1, 7), "combine", (1, 8), (1, 9), (2, "a"), (2, "b"), (1, 10)]
AFTER_SUM = [(1, 11), (1, 12), (2, 1), (2, 2), (1, 13), (1, 14), "relay", (2, 5), (2, 3), (2, 4), (1, 15)]
AMID_UP = [(2, 6), (2, 7)]
CHUNKS = ((0, 4), (4, 8), (8, 12), (12, 16))
TAIL = [
    "down0", (2, 8), (2, 9), "down1", (2, 11), (2, 12), "combine0", (2, 10), "down2", (2, 13), (2, 14), (2, 15), "combine1", "collect0",
    "down3", "combine2", "collect1", "combine3", "collect2", "collect3",
]


def kernel(
    qa_ref, ka_ref, va_ref, qb_ref, kb_ref, vb_ref, gqa_ref, gka_ref, gqb_ref, gkb_ref,
    ngain_ref, rowtab_ref, coltab_ref,
    resid_hbm, woa_hbm, wob_hbm, wup_hbm, wdown_hbm,
    out_ref,
    kvbuf, wbuf, wo, resid, qa, qb, s_even, s_odd, tops, acc_a, acc_b, attn,
    pout, phalf, rsbuf, nbuf, hidden, dbuf, dhalf, frecv, stage, midbuf,
    lsem, ssem, rsem, precv, xs, xr, gs, gr,
):
    sp = lax.axis_index("sp")
    x = lax.axis_index("tp")
    z, y, c = sp // 8, (sp // 2) % 4, sp % 2
    n = 1 - c
    partner = z * 8 + y * 2 + n

    def slot(da, db):
        return ((z + n * db + c * da) % 4) * 8 + ((y + n * da + c * db) % 4) * 2 + c

    def partner_slot(da, db):
        return ((z + c * db + n * da) % 4) * 8 + ((y + c * da + n * db) % 4) * 2 + n

    def event(da, db):
        return ORDER.index((da, db))

    barrier = pltpu.get_barrier_semaphore()
    others = [(slot(1, 0), x), (slot(3, 0), x), (slot(0, 1), x), (slot(0, 3), x), (partner, x)]
    others += [(sp, (x + d) % 4) for d in (1, 3)]
    for dev in others:
        pl.semaphore_signal(barrier, inc=1, device_id=dev, device_id_type=MESH)

    loads = [
        pltpu.make_async_copy(wup_hbm, wbuf.at[0, sp], lsem.at[0]),
        pltpu.make_async_copy(wdown_hbm, wbuf.at[1, sp], lsem.at[1]),
        pltpu.make_async_copy(woa_hbm, wo.at[pl.ds(0, 256)], lsem.at[2]),
        pltpu.make_async_copy(wob_hbm, wo.at[pl.ds(256, 256)], lsem.at[3]),
        pltpu.make_async_copy(resid_hbm, resid, lsem.at[4]),
    ]
    for load in loads:
        load.start()

    def region(item, index, half):
        if item == KV:
            ref, size = kvbuf.at[index], 384
        else:
            ref, size = wbuf.at[item - 1, index], 32
        if half is None:
            return ref
        return ref.at[pl.ds(half * size, size)]

    def block_copy(item, piece, recv_sem, to):
        return pltpu.make_async_remote_copy(
            src_ref=piece, dst_ref=piece, send_sem=ssem.at[item], recv_sem=recv_sem, device_id=(to, x), device_id_type=MESH,
        )

    def send(item, index, half, to, there):
        block_copy(item, region(item, index, half), rsem.at[item, event(*there)], slot(*to)).start()

    def hand_over(item, ev, index):
        block_copy(item, region(item, index, None), precv.at[item, ev], partner).start()

    def wait_in(item, ev, index):
        block_copy(item, region(item, index, None), rsem.at[item, ev], partner).wait_recv()

    def wait_partner(item, ev, index):
        block_copy(item, region(item, index, None), precv.at[item, ev], partner).wait_recv()

    def drain(item):
        ref = kvbuf.at[pl.ds(0, 31)] if item == KV else wbuf.at[item - 1, pl.ds(0, 31)]
        block_copy(item, ref, rsem.at[item, 0], partner).wait_send()

    def take(item, number):
        with jax.named_scope(f"take{item}_{number}"):
            if number in ("a", "b"):
                start_own(item, number)
            else:
                take_in(item, *ORDER[number])

    def start_own(item, ring):
        index = slot(0, 0)
        if ring == "a":
            send(item, index, None, (1, 0), (3, 0))
            send(item, index, None, (3, 0), (1, 0))
        else:
            send(item, index, None, (0, 1), (0, 3))
            send(item, index, None, (0, 3), (0, 1))
            hand_over(item, 0, index)

    def take_in(item, da, db):
        ev, index = event(da, db), slot(da, db)
        wait_in(item, ev, index)
        if db == 0:
            if da == 3:
                send(item, index, 0, (1, 0), (2, 0))
            elif da == 1:
                send(item, index, 1, (3, 0), (2, 0))
            send(item, index, None, (0, 1), (da, 3))
            send(item, index, None, (0, 3), (da, 1))
        elif db == 3:
            send(item, index, 0, (0, 1), (da, 2))
        elif db == 1:
            send(item, index, 1, (0, 3), (da, 2))
        hand_over(item, ev, index)

    with jax.named_scope("barrier"):
        pl.semaphore_wait(barrier, len(others))
    for to, there in (((1, 0), (3, 0)), ((3, 0), (1, 0))):
        pltpu.make_async_remote_copy(
            src_ref=wup_hbm, dst_ref=wbuf.at[0, sp], send_sem=ssem.at[UP], recv_sem=rsem.at[UP, event(*there)],
            device_id=(slot(*to), x), device_id_type=MESH,
        ).start()

    lane = lax.broadcasted_iota(jnp.int32, (64, 128), 1)
    low = lane < 64
    rowtab = rowtab_ref[sp]

    def both_heads(ref):
        return jnp.concatenate([ref[...], ref[...]], axis=1)

    def rotate(v, gain, width, r, s):
        quarter = width // 4
        kind = 0 if width == 64 else 2

        def angles(which):
            across = rowtab[which * 4 + r : which * 4 + r + 1]
            if s != r:
                across = jnp.where(low[0:1], across, rowtab[which * 4 + s : which * 4 + s + 1])
            return across + coltab_ref[which]

        sq = v * v
        if width == 64:
            left = jnp.sum(jnp.where(low, sq, 0.0), axis=-1, keepdims=True)
            right = jnp.sum(jnp.where(low, 0.0, sq), axis=-1, keepdims=True)
            mean = jnp.where(low, left, right) * (1.0 / 64)
        else:
            mean = jnp.sum(sq, axis=-1, keepdims=True) * (1.0 / 128)
        u = v * lax.rsqrt(mean + EPS) * gain
        even = (lane // quarter) % 2 == 0
        turned = jnp.where(even, pltpu.roll(u, 128 - quarter, 1), pltpu.roll(u, quarter, 1))
        return u * angles(kind) + turned * angles(kind + 1)

    own = slot(0, 0)
    turned = ka_ref[...].astype(F32)
    turned = jnp.concatenate([turned[:, 0:128], turned[:, 128:256]], axis=0).T
    gain = both_heads(gka_ref)
    for r in range(2):
        block = rotate(turned[r * 64 : (r + 1) * 64], gain, 64, r, r + 2)
        kvbuf[own, r * 64 : (r + 1) * 64, :] = block.astype(BF16)
    for r in range(4):
        block = rotate(kb_ref[r * 64 : (r + 1) * 64, :].astype(F32), gkb_ref[...], 128, r, r)
        kvbuf[own, 128 + r * 64 : 192 + r * 64, :] = block.astype(BF16)
    for half in range(2):
        tokens = slice(half * 128, half * 128 + 128)
        kvbuf[own, 384 + half * 64 : 448 + half * 64, :] = va_ref[:, tokens]
        kvbuf[own, 512 + half * 128 : 640 + half * 128, :] = vb_ref[tokens, :].astype(F32).T.astype(BF16)

    take(KV, "a")
    take(KV, "b")
    loads[0].wait()

    with jax.named_scope("queries"):
        gain_a = both_heads(gqa_ref)
        for g in range(2):
            lanes = slice(g * 128, g * 128 + 128)
            rows = [slice(r * 64, r * 64 + 64) for r in range(4)]
            heads = [rotate(qa_ref[rows[r], lanes].astype(F32), gain_a, 64, r, r) for r in range(4)]
            heads = jnp.concatenate(heads, axis=0).T.astype(BF16)
            for h in range(2):
                head = heads[h * 64 : h * 64 + 64]
                qa[2 * g + h, 0:64, 0:256] = head
                qa[2 * g + h, 0:64, 256:512] = jnp.zeros_like(head)
                qa[2 * g + h, 64:128, 0:256] = jnp.zeros_like(head)
                qa[2 * g + h, 64:128, 256:512] = head
            heads = [rotate(qb_ref[rows[r], lanes].astype(F32), gqb_ref[...], 128, r, r) for r in range(4)]
            qb[g] = jnp.concatenate(heads, axis=0).T.astype(BF16)
        tops[...] = jnp.full_like(tops, -1e30)
        acc_a[...] = jnp.zeros_like(acc_a)
        acc_b[...] = jnp.zeros_like(acc_b)

    scale_a = 64 ** (-0.5) * LOG2E
    scale_b = 128 ** (-0.5) * LOG2E

    def turned_values(pieces):
        values = jnp.concatenate(pieces, axis=1)
        return jnp.concatenate([values, jnp.ones((16, 512), BF16)], axis=0)

    def score(pair, target):
        keys_a = jnp.concatenate([kvbuf[s, 0:128, :] for s in pair], axis=0)
        keys_b = jnp.concatenate([kvbuf[s, 128:384, :] for s in pair], axis=0)

        def one(h):
            if h < 4:
                scores = nn_dot(keys_a, qa[h]) * scale_a
                scores = jnp.concatenate([scores[:, 0:256], scores[:, 256:512]], axis=0)
            else:
                scores = nn_dot(keys_b, qb[h - 4]) * scale_b
            target[h] = scores
            before = tops[h, 0:1, :]
            top = jnp.maximum(before, jnp.max(scores, axis=0, keepdims=True))
            tops[h, 0:1, :] = top
            tops[h, 1:2, :] = jnp.exp2(before - top)

        return one

    def gather_values(pair):
        def one(h):
            if h < 4:
                return turned_values([kvbuf[s, 384 + 64 * half : 448 + 64 * half, :] for half in range(2) for s in pair])
            return turned_values([kvbuf[s, 512 + 128 * half : 640 + 128 * half, :] for s in pair for half in range(2)])

        return one(0), one(4)

    def use(source, h, values, top, factor):
        expo = jnp.exp2(source[h] - top).astype(BF16)
        got = nn_dot(values[0] if h < 4 else values[1], expo)
        acc, index = (acc_a, h) if h < 4 else (acc_b, h - 4)
        acc[index] = acc[index] * factor + got

    def both(now, after, source, target):
        values = gather_values(now)
        scorer = None if after is None else score(after, target)
        for h in range(6):
            top, factor = tops[h, 0:1, :], tops[h, 1:2, :]
            if scorer is not None:
                scorer(h)
            use(source, h, values, top, factor)

    def my_block(t, shift):
        places = ORDER[shift::2]
        return slot(pick(t, [p[0] for p in places]), pick(t, [p[1] for p in places]))

    def partner_block(t, shift):
        places = ORDER[shift::2]
        return partner_slot(pick(t, [p[0] for p in places]), pick(t, [p[1] for p in places]))

    def ready(t, shift):
        for number in range(6):
            if PLAN.get(2 * number + shift):

                @pl.when(t == number)
                def _(number=number):
                    for what in PLAN[2 * number + shift]:
                        take(*what)

    def fetch(number, t, shift):
        theirs = partner_block(t, shift - 1)
        with jax.named_scope("pwait"):
            wait_partner(KV, number - 1, theirs)
        return my_block(t, shift + 1), theirs

    def attend(t, pair):
        with jax.named_scope("step"):
            ready(t, 2)
            middle = fetch(2 * t + 2, t, 2)
            both(pair, middle, s_odd, s_even)
            ready(t, 3)
            after = fetch(2 * t + 3, t, 3)
            both(middle, after, s_even, s_odd)
        return after

    loads[1].wait()
    with jax.named_scope("first"):
        wait_partner(KV, 0, partner)
        pair = (own, partner)
        first = score(pair, s_even)
        for h in range(6):
            first(h)
        for what in PLAN[1]:
            take(*what)
        after = (slot(*ORDER[1]), slot(*ORDER[2]))
        both(pair, after, s_even, s_odd)
    pair = lax.fori_loop(0, 6, attend, after)
    with jax.named_scope("laststep"):
        for what in PLAN[14]:
            take(*what)
        theirs = partner_slot(*ORDER[13])
        wait_partner(KV, 13, theirs)
        middle = (slot(*ORDER[15]), theirs)
        both(pair, middle, s_odd, s_even)
        for what in PLAN[15]:
            take(*what)
        after = (partner_slot(*ORDER[14]), partner_slot(*ORDER[15]))
        wait_partner(KV, 14, after[0])
        wait_partner(KV, 15, after[1])
        both(middle, after, s_even, s_odd)
        both(after, None, s_odd, None)
        for what in PLAN[16]:
            take(*what)

    for h in range(4):
        acc = acc_a[h]
        acc_a[h, 0:64, :] = acc[0:64] / acc[64:65]
    for g in range(2):
        both_rows = jnp.concatenate([acc_a[2 * g, 0:64, :], acc_a[2 * g + 1, 0:64, :]], axis=0)
        attn[:, g * 128 : (g + 1) * 128] = both_rows.T.astype(BF16)
        acc = acc_b[g]
        attn[:, 256 + g * 128 : 256 + (g + 1) * 128] = (acc[0:128] / acc[128:129]).T.astype(BF16)
    loads[2].wait()
    loads[3].wait()

    def project(j, carry):
        cols = pl.ds(pl.multiple_of(j * 512, 512), 512)
        part = jnp.dot(attn[...], wo[:, cols], preferred_element_type=F32).astype(BF16)
        for r in range(4):
            pout[r, :, cols] = part[r * 64 : (r + 1) * 64, :]
        return carry

    with jax.named_scope("project"):
        lax.fori_loop(0, 4, project, 0)

    def to_peer(forward, src, dst, send_sem, recv_sem):
        return pltpu.make_async_remote_copy(
            src_ref=src,
            dst_ref=dst,
            send_sem=send_sem,
            recv_sem=recv_sem,
            device_id=(sp, (x + (1 if forward else 3)) % 4),
            device_id_type=MESH,
        )

    class TpSum:
        def __init__(self, number, blocks, halves, received):
            self.number, self.blocks, self.halves, self.received = number, blocks, halves, received
            width = received(0).shape[1] // 2
            self.parts = (pl.ds(0, width), pl.ds(width, width))

        def copy(self, kind, way):
            near = self.blocks((x + (1, 3)[way]) % 4)
            if kind == 0:
                src, dst = self.blocks((x + 2) % 4).at[:, self.parts[way]], self.halves(way)
            else:
                part = self.parts[1 - way] if kind == 1 else self.parts[way]
                src, dst = near.at[:, part], self.received(way).at[:, part]
            return to_peer(way == 0, src, dst, xs.at[min(self.number, 1)], xr.at[self.number, min(kind, 1), way])

        def start(self):
            for kind in (0, 1):
                for way in (0, 1):
                    self.copy(kind, way).start()

        def combine(self):
            for way in (0, 1):
                self.copy(0, way).wait_recv()
                near, part = self.blocks((x + (1, 3)[way]) % 4), self.parts[way]
                near[:, part] = (near[:, part].astype(F32) + self.halves(way)[...].astype(F32)).astype(BF16)
                self.copy(2, way).start()

        def total(self):
            for way in (0, 1):
                block = self.received(way)
                to_peer(True, block, block, xs.at[0], xr.at[self.number, 1, way]).wait_recv()
            return self.blocks(x)[...].astype(F32) + self.received(0)[...].astype(F32) + self.received(1)[...].astype(F32)

    def drain_tp(ref, sem):
        three = ref.at[pl.ds(0, 3)]
        to_peer(True, three, three, sem, xr.at[0, 0, 0]).wait_send()

    proj = TpSum(0, lambda r: pout.at[r], lambda w: phalf.at[w], lambda w: rsbuf.at[w])
    proj.start()
    for what in AFTER_PROJECT:
        if what == "combine":
            with jax.named_scope("combine"):
                proj.combine()
        else:
            take(*what)
    loads[4].wait()
    with jax.named_scope("rswait"):
        total = proj.total()
    mid = (resid[...].astype(F32) + total).astype(BF16).astype(F32)
    midbuf[...] = mid
    norm = mid * lax.rsqrt(jnp.mean(mid * mid, axis=-1, keepdims=True) + EPS) * ngain_ref[...]
    nbuf[x] = norm.astype(BF16)

    halves = (pl.ds(0, 1024), pl.ds(1024, 1024))

    def rows_copy(kind, way, arriving):
        hops = (1 if kind < 2 else 2) if arriving else (0 if kind < 2 else 1)
        block = (x + 4 - hops) % 4 if way == 0 else (x + hops) % 4
        part = halves[1 - way] if kind == 1 else halves[way]
        piece = nbuf.at[block, :, part]
        return to_peer(way == 0, piece, piece, gs.at[0], gr.at[kind, way])

    for kind in (0, 1):
        for way in (0, 1):
            rows_copy(kind, way, False).start()
    for what in AFTER_SUM:
        if what == "relay":
            with jax.named_scope("relay"):
                for way in (0, 1):
                    rows_copy(0, way, True).wait_recv()
                    rows_copy(2, way, False).start()
        else:
            take(*what)
    with jax.named_scope("upwait"):
        for ev in range(16):
            wait_partner(UP, ev, partner_slot(*ORDER[ev]))
    with jax.named_scope("drainkv"):
        drain(KV)
    with jax.named_scope("rowswait"):
        for kind in (1, 2):
            for way in (0, 1):
                rows_copy(kind, way, True).wait_recv()

    def up(j, carry):
        cols = pl.ds(pl.multiple_of(j * 512, 512), 512)
        rows = nbuf[...].reshape(256, 2048)
        weights = wbuf[0, :, :, cols].reshape(2048, 512)
        part = jnp.maximum(jnp.dot(rows, weights, preferred_element_type=F32), 0.0)
        hidden[:, cols] = (part * part).astype(BF16)
        return carry

    with jax.named_scope("up"):
        lax.fori_loop(0, 2, up, 0)
    for what in AMID_UP:
        take(*what)
    with jax.named_scope("up"):
        lax.fori_loop(2, 4, up, 0)

    def chunk_sum(k):
        low_, high = CHUNKS[k]
        cols = pl.ds(low_ * 128, (high - low_) * 128)
        part = pl.ds(low_ * 64, (high - low_) * 64)
        return TpSum(k + 1, lambda r: dbuf.at[r, :, cols], lambda w: dhalf.at[w, :, part], lambda w: frecv.at[w, :, cols])

    sums = [chunk_sum(k) for k in range(len(CHUNKS))]

    def collect(k):
        total = sums[k].total()
        places = ORDER[slice(*CHUNKS[k])]
        blocks = [slot(*place) for place in places] + [partner_slot(*place) for place in places]
        for b, block in enumerate(blocks):
            piece = total[:, (b // 2) * 128 : (b // 2) * 128 + 128]
            if b % 2 == 1:
                piece = pltpu.roll(piece, 64, 1)
            stage[block] = piece

    def down(k):
        first_, last_ = CHUNKS[k]
        places = ORDER[first_:last_]
        with jax.named_scope("dwait"):
            for r in range(first_, last_):
                wait_partner(DOWN, r, partner_slot(*ORDER[r]))
        blocks = [slot(*place) for place in places] + [partner_slot(*place) for place in places]
        part = nt_dot(hidden[...], jnp.concatenate([wbuf[1, b] for b in blocks], axis=0)).astype(BF16)
        for r in range(4):
            dbuf[r, :, first_ * 128 : last_ * 128] = part[r * 64 : (r + 1) * 64, :]
        sums[k].start()

    for what in TAIL:
        if isinstance(what, tuple):
            take(*what)
        else:
            with jax.named_scope(what):
                kind, k = what[:-1], int(what[-1])
                if kind == "down":
                    down(k)
                elif kind == "combine":
                    sums[k].combine()
                else:
                    collect(k)
    drain(UP)
    drain(DOWN)
    drain_tp(pout, xs.at[0])
    drain_tp(nbuf, gs.at[0])
    with jax.named_scope("assemble"):
        for pos in range(16):
            both_halves = jnp.where(low, stage[2 * pos], pltpu.roll(stage[2 * pos + 1], 64, 1))
            cols = slice(pos * 128, pos * 128 + 128)
            out_ref[:, cols] = (midbuf[:, cols] + both_halves).astype(BF16)

    with jax.named_scope("draintp"):
        drain_tp(dbuf, xs.at[1])


def local(
    resid, query_a, key_a, value_a, query_b, key_b, value_b, gain_qa, gain_ka, gain_qb, gain_kb,
    w_out_a, w_out_b, norm_gain, w_up, w_down,
):
    rowtab, coltab = build_tables()
    vmem = pl.BlockSpec(memory_space=pltpu.VMEM)
    anywhere = pl.BlockSpec(memory_space=pl.ANY)
    dma = pltpu.SemaphoreType.DMA
    return pl.pallas_call(
        kernel,
        out_shape=pltpu.VMEM((64, 2048), BF16),
        in_specs=[vmem] * 13 + [anywhere] * 5,
        out_specs=vmem,
        scratch_shapes=[
            pltpu.VMEM((32, 768, 128), BF16),
            pltpu.VMEM((2, 32, 64, 2048), BF16),
            pltpu.VMEM((512, 2048), BF16),
            pltpu.VMEM((64, 2048), BF16),
            pltpu.VMEM((4, 128, 512), BF16),
            pltpu.VMEM((2, 128, 256), BF16),
            pltpu.VMEM((6, 512, 256), F32),
            pltpu.VMEM((6, 512, 256), F32),
            pltpu.VMEM((6, 8, 256), F32),
            pltpu.VMEM((4, 80, 256), F32),
            pltpu.VMEM((2, 144, 256), F32),
            pltpu.VMEM((256, 512), BF16),
            pltpu.VMEM((4, 64, 2048), BF16),
            pltpu.VMEM((2, 64, 1024), BF16),
            pltpu.VMEM((2, 64, 2048), BF16),
            pltpu.VMEM((4, 64, 2048), BF16),
            pltpu.VMEM((256, 2048), BF16),
            pltpu.VMEM((4, 64, 2048), BF16),
            pltpu.VMEM((2, 64, 1024), BF16),
            pltpu.VMEM((2, 64, 2048), BF16),
            pltpu.VMEM((32, 64, 128), F32),
            pltpu.VMEM((64, 2048), F32),
            dma((5,)),
            dma((3,)),
            dma((3, 16)),
            dma((3, 16)),
            dma((2,)),
            dma((5, 2, 2)),
            dma((1,)),
            dma((3, 2)),
        ],
        compiler_params=pltpu.CompilerParams(
            collective_id=0, has_side_effects=True, vmem_limit_bytes=58 * 1024 * 1024
        ),
    )(
        query_a, key_a.T, value_a.T, query_b, key_b, value_b,
        gain_qa.reshape(1, -1), gain_ka.reshape(1, -1), gain_qb.reshape(1, -1), gain_kb.reshape(1, -1),
        norm_gain.reshape(1, -1), jnp.asarray(rowtab), jnp.asarray(coltab),
        resid, w_out_a, w_out_b, w_up, w_down.T,
    )


def solution(mesh):
    return jax.shard_map(
        local,
        mesh=mesh,
        in_specs=(
            P(("sp", "tp"), None),
            P("sp", "tp"),
            P("sp", "tp"),
            P("sp", "tp"),
            P("sp", "tp"),
            P("sp", "tp"),
            P("sp", "tp"),
            P(),
            P(),
            P(),
            P(),
            P("tp", None),
            P("tp", None),
            P(),
            P("sp", "tp"),
            P("tp", "sp"),
        ),
        out_specs=P(("sp", "tp"), None),
        check_vma=False,
    )
```

```python
import functools
import math

import jax
import jax.numpy as jnp
import numpy as np
from jax import lax
from jax.experimental import pallas as pl
from jax.experimental.pallas import tpu as pltpu
from jax.sharding import PartitionSpec as P

MESH = pl.DeviceIdType.MESH
EPS = 1e-06
F32 = jnp.float32
BF16 = jnp.bfloat16
LOG2E = 1.4426950408889634
KV, UP, DOWN = 0, 1, 2
ORDER = (
    (0, 0), (3, 0), (1, 0), (0, 3), (0, 1), (2, 0), (3, 3), (3, 1),
    (1, 3), (1, 1), (0, 2), (2, 3), (2, 1), (3, 2), (1, 2), (2, 2),
)


def build_tables():
    rows, cols = [], []
    for width in (64, 128):
        quarter = width // 4
        freqs = (10000.0 ** (-(2.0 * np.arange(quarter)) / (width // 2))).astype(np.float32)
        freqs = np.concatenate([freqs, freqs])
        entry = np.arange(width)
        sign = np.where((entry // quarter) % 2 == 0, -1.0, 1.0)

        def pair(count, low):
            ang = (np.arange(count, dtype=np.float32)[:, None] * freqs).astype(np.float64)
            full = np.zeros((2, count, width))
            half = slice(0, width // 2) if low else slice(width // 2, width)
            full[0][:, half] = np.cos(ang)
            full[1][:, half] = np.sin(ang)
            full[1] *= sign
            return np.tile(full, (1, 1, 128 // width)).astype(np.float32)

        rows.append(pair(128, True))
        cols.append(pair(64, False))
    row = np.concatenate(rows, axis=0)
    row = row.reshape(4, 32, 4, 128).transpose(1, 0, 2, 3).reshape(32, 16, 128)
    col = np.concatenate(cols, axis=0)
    return row, col


def nt_dot(a, b):
    return lax.dot_general(a, b, (((1,), (1,)), ((), ())), preferred_element_type=F32)


def nn_dot(a, b):
    return jnp.dot(a, b, preferred_element_type=F32)


def pick(i, values):
    result = jnp.int32(values[0])
    for number, value in enumerate(values[1:]):
        result = jnp.where(i == number + 1, jnp.int32(value), result)
    return result


PLAN = {
    1: [(0, 1), (0, 2), (0, 3), (0, 4)],
    4: [(0, 5)],
    5: [(0, 6), (0, 7)],
    7: [(0, 8), (0, 9)],
    8: [(0, 10)],
    10: [(0, 11), (0, 12)],
    11: [(0, 13), (1, "b")],
    12: [(0, 14)],
    14: [(0, 15), (1, 1), (1, 2)],
    15: [],
    16: [(1, 3), (1, 4)],
}
AFTER_PROJECT = [(1, 5), (1, 6), (1, 7), (2, "a"), (2, "b"), "combine", (1, 8), (1, 9), (1, 10)]
AFTER_SUM = [(1, 11), (1, 12), (2, 1), (2, 2), (1, 13), "relay", (1, 14), (2, 5), (2, 3), (2, 4), (1, 15)]
AMID_UP = [(2, 6), (2, 7)]
CHUNKS = ((0, 4), (4, 8), (8, 12), (12, 14), (14, 16))
TAIL = [
    "down0", (2, 8), (2, 9), "down1", (2, 11), (2, 12), "combine0", (2, 10), "down2", (2, 13), (2, 14), "combine1", "collect0",
    "down3", (2, 15), "combine2", "down4", "collect1", "combine3", "collect2", "collect3", "collect4",
]


def kernel(
    qa_ref, ka_ref, va_ref, qb_ref, kb_ref, vb_ref, gqa_ref, gka_ref, gqb_ref, gkb_ref,
    ngain_ref, rowtab_ref, coltab_ref,
    resid_hbm, woa_hbm, wob_hbm, wup_hbm, wdown_hbm,
    out_ref,
    kvbuf, wbuf, wo, resid, qa, qb, s_even, s_odd, tops, acc_a, acc_b, attn,
    pout, phalf, rsbuf, nbuf, hidden, dbuf, dhalf, frecv, stage, midbuf, lastbuf,
    lsem, ssem, rsem, precv, xs, xr, gs, gr, lr,
):
    sp = lax.axis_index("sp")
    x = lax.axis_index("tp")
    z, y, c = sp // 8, (sp // 2) % 4, sp % 2
    n = 1 - c
    partner = z * 8 + y * 2 + n

    def slot(da, db):
        return ((z + n * db + c * da) % 4) * 8 + ((y + n * da + c * db) % 4) * 2 + c

    def partner_slot(da, db):
        return ((z + c * db + n * da) % 4) * 8 + ((y + c * da + n * db) % 4) * 2 + n

    def event(da, db):
        return ORDER.index((da, db))

    barrier = pltpu.get_barrier_semaphore()
    others = [(slot(1, 0), x), (slot(3, 0), x), (slot(0, 1), x), (slot(0, 3), x), (partner, x)]
    others += [(sp, (x + d) % 4) for d in (1, 2, 3)]
    for dev in others:
        pl.semaphore_signal(barrier, inc=1, device_id=dev, device_id_type=MESH)

    loads = [
        pltpu.make_async_copy(wup_hbm, wbuf.at[0, sp], lsem.at[0]),
        pltpu.make_async_copy(wdown_hbm, wbuf.at[1, sp], lsem.at[1]),
        pltpu.make_async_copy(woa_hbm, wo.at[pl.ds(0, 256)], lsem.at[2]),
        pltpu.make_async_copy(wob_hbm, wo.at[pl.ds(256, 256)], lsem.at[3]),
        pltpu.make_async_copy(resid_hbm, resid, lsem.at[4]),
    ]
    for load in loads:
        load.start()

    def region(item, index, half):
        if item == KV:
            ref, size = kvbuf.at[index], 384
        else:
            ref, size = wbuf.at[item - 1, index], 32
        if half is None:
            return ref
        return ref.at[pl.ds(half * size, size)]

    def block_copy(item, piece, recv_sem, to):
        return pltpu.make_async_remote_copy(
            src_ref=piece, dst_ref=piece, send_sem=ssem.at[item], recv_sem=recv_sem, device_id=(to, x), device_id_type=MESH,
        )

    def send(item, index, half, to, there):
        block_copy(item, region(item, index, half), rsem.at[item, event(*there)], slot(*to)).start()

    def hand_over(item, ev, index):
        block_copy(item, region(item, index, None), precv.at[item, ev], partner).start()

    def wait_in(item, ev, index):
        block_copy(item, region(item, index, None), rsem.at[item, ev], partner).wait_recv()

    def wait_partner(item, ev, index):
        block_copy(item, region(item, index, None), precv.at[item, ev], partner).wait_recv()

    def drain(item):
        ref = kvbuf.at[pl.ds(0, 31)] if item == KV else wbuf.at[item - 1, pl.ds(0, 31)]
        block_copy(item, ref, rsem.at[item, 0], partner).wait_send()

    def take(item, number):
        with jax.named_scope(f"take{item}_{number}"):
            if number in ("a", "b"):
                start_own(item, number)
            else:
                take_in(item, *ORDER[number])

    def start_own(item, ring):
        index = slot(0, 0)
        if ring == "a":
            send(item, index, None, (1, 0), (3, 0))
            send(item, index, None, (3, 0), (1, 0))
        else:
            send(item, index, None, (0, 1), (0, 3))
            send(item, index, None, (0, 3), (0, 1))
            hand_over(item, 0, index)

    def take_in(item, da, db):
        ev, index = event(da, db), slot(da, db)
        wait_in(item, ev, index)
        if db == 0:
            if da == 3:
                send(item, index, 0, (1, 0), (2, 0))
            elif da == 1:
                send(item, index, 1, (3, 0), (2, 0))
            send(item, index, None, (0, 1), (da, 3))
            send(item, index, None, (0, 3), (da, 1))
        elif db == 3:
            send(item, index, 0, (0, 1), (da, 2))
        elif db == 1:
            send(item, index, 1, (0, 3), (da, 2))
        hand_over(item, ev, index)

    def own_up(half):
        part = pl.ds(half * 32, 32)
        for to, there in (((1, 0), (3, 0)), ((3, 0), (1, 0))):
            pltpu.make_async_remote_copy(
                src_ref=wup_hbm.at[part], dst_ref=wbuf.at[0, sp, part], send_sem=ssem.at[UP], recv_sem=rsem.at[UP, event(*there)],
                device_id=(slot(*to), x), device_id_type=MESH,
            ).start()

    with jax.named_scope("barrier"):
        pl.semaphore_wait(barrier, len(others))
    own_up(0)

    lane = lax.broadcasted_iota(jnp.int32, (64, 128), 1)
    low = lane < 64
    rowtab = rowtab_ref[sp]

    def both_heads(ref):
        return jnp.concatenate([ref[...], ref[...]], axis=1)

    def rotate(v, gain, width, r, s):
        quarter = width // 4
        kind = 0 if width == 64 else 2

        def angles(which):
            across = rowtab[which * 4 + r : which * 4 + r + 1]
            if s != r:
                across = jnp.where(low[0:1], across, rowtab[which * 4 + s : which * 4 + s + 1])
            return across + coltab_ref[which]

        sq = v * v
        if width == 64:
            left = jnp.sum(jnp.where(low, sq, 0.0), axis=-1, keepdims=True)
            right = jnp.sum(jnp.where(low, 0.0, sq), axis=-1, keepdims=True)
            mean = jnp.where(low, left, right) * (1.0 / 64)
        else:
            mean = jnp.sum(sq, axis=-1, keepdims=True) * (1.0 / 128)
        u = v * lax.rsqrt(mean + EPS) * gain
        even = (lane // quarter) % 2 == 0
        turned = jnp.where(even, pltpu.roll(u, 128 - quarter, 1), pltpu.roll(u, quarter, 1))
        return u * angles(kind) + turned * angles(kind + 1)

    own = slot(0, 0)
    turned = ka_ref[...].astype(F32)
    turned = jnp.concatenate([turned[:, 0:128], turned[:, 128:256]], axis=0).T
    gain = both_heads(gka_ref)
    for r in range(2):
        block = rotate(turned[r * 64 : (r + 1) * 64], gain, 64, r, r + 2)
        kvbuf[own, r * 64 : (r + 1) * 64, :] = block.astype(BF16)
    for r in range(4):
        block = rotate(kb_ref[r * 64 : (r + 1) * 64, :].astype(F32), gkb_ref[...], 128, r, r)
        kvbuf[own, 128 + r * 64 : 192 + r * 64, :] = block.astype(BF16)
    for half in range(2):
        tokens = slice(half * 128, half * 128 + 128)
        kvbuf[own, 384 + half * 64 : 448 + half * 64, :] = va_ref[:, tokens]
        kvbuf[own, 512 + half * 128 : 640 + half * 128, :] = vb_ref[tokens, :].astype(F32).T.astype(BF16)

    take(KV, "a")
    take(KV, "b")
    loads[0].wait()
    own_up(1)

    with jax.named_scope("queries"):
        gain_a = both_heads(gqa_ref)
        for g in range(2):
            lanes = slice(g * 128, g * 128 + 128)
            rows = [slice(r * 64, r * 64 + 64) for r in range(4)]
            heads = [rotate(qa_ref[rows[r], lanes].astype(F32), gain_a, 64, r, r) for r in range(4)]
            heads = jnp.concatenate(heads, axis=0).T.astype(BF16)
            for h in range(2):
                head = heads[h * 64 : h * 64 + 64]
                qa[2 * g + h, 0:64, 0:256] = head
                qa[2 * g + h, 0:64, 256:512] = jnp.zeros_like(head)
                qa[2 * g + h, 64:128, 0:256] = jnp.zeros_like(head)
                qa[2 * g + h, 64:128, 256:512] = head
            heads = [rotate(qb_ref[rows[r], lanes].astype(F32), gqb_ref[...], 128, r, r) for r in range(4)]
            qb[g] = jnp.concatenate(heads, axis=0).T.astype(BF16)
        tops[...] = jnp.full_like(tops, -1e30)
        acc_a[...] = jnp.zeros_like(acc_a)
        acc_b[...] = jnp.zeros_like(acc_b)

    scale_a = 64 ** (-0.5) * LOG2E
    scale_b = 128 ** (-0.5) * LOG2E

    def turned_values(pieces):
        values = jnp.concatenate(pieces, axis=1)
        return jnp.concatenate([values, jnp.ones((16, 512), BF16)], axis=0)

    def score(pair, target):
        keys_a = jnp.concatenate([kvbuf[s, 0:128, :] for s in pair], axis=0)
        keys_b = jnp.concatenate([kvbuf[s, 128:384, :] for s in pair], axis=0)

        def one(h):
            if h < 4:
                scores = nn_dot(keys_a, qa[h]) * scale_a
                scores = jnp.concatenate([scores[:, 0:256], scores[:, 256:512]], axis=0)
            else:
                scores = nn_dot(keys_b, qb[h - 4]) * scale_b
            target[h] = scores
            before = tops[h, 0:1, :]
            top = jnp.maximum(before, jnp.max(scores, axis=0, keepdims=True))
            tops[h, 0:1, :] = top
            tops[h, 1:2, :] = jnp.exp2(before - top)

        return one

    def gather_values(pair):
        def one(h):
            if h < 4:
                return turned_values([kvbuf[s, 384 + 64 * half : 448 + 64 * half, :] for half in range(2) for s in pair])
            return turned_values([kvbuf[s, 512 + 128 * half : 640 + 128 * half, :] for s in pair for half in range(2)])

        return one(0), one(4)

    def use(source, h, values, top, factor):
        expo = jnp.exp2(source[h] - top).astype(BF16)
        got = nn_dot(values[0] if h < 4 else values[1], expo)
        acc, index = (acc_a, h) if h < 4 else (acc_b, h - 4)
        acc[index] = acc[index] * factor + got

    def both(now, after, source, target):
        values = gather_values(now)
        scorer = None if after is None else score(after, target)
        for h in range(6):
            top, factor = tops[h, 0:1, :], tops[h, 1:2, :]
            if scorer is not None:
                scorer(h)
            use(source, h, values, top, factor)

    def my_block(t, shift):
        places = ORDER[shift::2]
        return slot(pick(t, [p[0] for p in places]), pick(t, [p[1] for p in places]))

    def partner_block(t, shift):
        places = ORDER[shift::2]
        return partner_slot(pick(t, [p[0] for p in places]), pick(t, [p[1] for p in places]))

    def ready(t, shift):
        for number in range(6):
            if PLAN.get(2 * number + shift):

                @pl.when(t == number)
                def _(number=number):
                    for what in PLAN[2 * number + shift]:
                        take(*what)

    def fetch(number, t, shift):
        theirs = partner_block(t, shift - 1)
        with jax.named_scope("pwait"):
            wait_partner(KV, number - 1, theirs)
        return my_block(t, shift + 1), theirs

    def attend(t, pair):
        with jax.named_scope("step"):
            ready(t, 2)
            middle = fetch(2 * t + 2, t, 2)
            both(pair, middle, s_odd, s_even)
            ready(t, 3)
            after = fetch(2 * t + 3, t, 3)
            both(middle, after, s_even, s_odd)
        return after

    loads[1].wait()
    with jax.named_scope("first"):
        wait_partner(KV, 0, partner)
        pair = (own, partner)
        first = score(pair, s_even)
        for h in range(6):
            first(h)
        for what in PLAN[1]:
            take(*what)
        after = (slot(*ORDER[1]), slot(*ORDER[2]))
        both(pair, after, s_even, s_odd)
    pair = lax.fori_loop(0, 6, attend, after)
    with jax.named_scope("laststep"):
        for what in PLAN[14]:
            take(*what)
        theirs = partner_slot(*ORDER[13])
        wait_partner(KV, 13, theirs)
        middle = (slot(*ORDER[15]), theirs)
        both(pair, middle, s_odd, s_even)
        for what in PLAN[15]:
            take(*what)
        after = (partner_slot(*ORDER[14]), partner_slot(*ORDER[15]))
        wait_partner(KV, 14, after[0])
        wait_partner(KV, 15, after[1])
        both(middle, after, s_even, s_odd)
        both(after, None, s_odd, None)
        for what in PLAN[16]:
            take(*what)

    for h in range(4):
        acc = acc_a[h]
        acc_a[h, 0:64, :] = acc[0:64] / acc[64:65]
    for g in range(2):
        both_rows = jnp.concatenate([acc_a[2 * g, 0:64, :], acc_a[2 * g + 1, 0:64, :]], axis=0)
        attn[:, g * 128 : (g + 1) * 128] = both_rows.T.astype(BF16)
        acc = acc_b[g]
        attn[:, 256 + g * 128 : 256 + (g + 1) * 128] = (acc[0:128] / acc[128:129]).T.astype(BF16)
    loads[2].wait()
    loads[3].wait()

    def project(j, carry):
        cols = pl.ds(pl.multiple_of(j * 512, 512), 512)
        part = jnp.dot(attn[...], wo[:, cols], preferred_element_type=F32).astype(BF16)
        for r in range(4):
            pout[r, :, cols] = part[r * 64 : (r + 1) * 64, :]
        return carry

    with jax.named_scope("project"):
        lax.fori_loop(0, 4, project, 0)

    def to_peer(forward, src, dst, send_sem, recv_sem):
        return pltpu.make_async_remote_copy(
            src_ref=src,
            dst_ref=dst,
            send_sem=send_sem,
            recv_sem=recv_sem,
            device_id=(sp, (x + (1 if forward else 3)) % 4),
            device_id_type=MESH,
        )

    class TpSum:
        def __init__(self, number, blocks, halves, received):
            self.number, self.blocks, self.halves, self.received = number, blocks, halves, received
            width = received(0).shape[1] // 2
            self.parts = (pl.ds(0, width), pl.ds(width, width))

        def copy(self, kind, way):
            near = self.blocks((x + (1, 3)[way]) % 4)
            if kind == 0:
                src, dst = self.blocks((x + 2) % 4).at[:, self.parts[way]], self.halves(way)
            else:
                part = self.parts[1 - way] if kind == 1 else self.parts[way]
                src, dst = near.at[:, part], self.received(way).at[:, part]
            return to_peer(way == 0, src, dst, xs.at[min(self.number, 1)], xr.at[self.number, min(kind, 1), way])

        def start(self):
            for kind in (0, 1):
                for way in (0, 1):
                    self.copy(kind, way).start()

        def combine(self):
            for way in (0, 1):
                self.copy(0, way).wait_recv()
                near, part = self.blocks((x + (1, 3)[way]) % 4), self.parts[way]
                near[:, part] = (near[:, part].astype(F32) + self.halves(way)[...].astype(F32)).astype(BF16)
                self.copy(2, way).start()

        def total(self):
            for way in (0, 1):
                block = self.received(way)
                to_peer(True, block, block, xs.at[0], xr.at[self.number, 1, way]).wait_recv()
            return self.blocks(x)[...].astype(F32) + self.received(0)[...].astype(F32) + self.received(1)[...].astype(F32)

    def drain_tp(ref, sem):
        three = ref.at[pl.ds(0, 3)]
        to_peer(True, three, three, sem, xr.at[0, 0, 0]).wait_send()

    proj = TpSum(0, lambda r: pout.at[r], lambda w: phalf.at[w], lambda w: rsbuf.at[w])
    proj.start()
    for what in AFTER_PROJECT:
        if what == "combine":
            with jax.named_scope("combine"):
                proj.combine()
        else:
            take(*what)
    loads[4].wait()
    with jax.named_scope("rswait"):
        total = proj.total()
    mid = (resid[...].astype(F32) + total).astype(BF16).astype(F32)
    midbuf[...] = mid
    norm = mid * lax.rsqrt(jnp.mean(mid * mid, axis=-1, keepdims=True) + EPS) * ngain_ref[...]
    nbuf[x] = norm.astype(BF16)

    halves = (pl.ds(0, 1024), pl.ds(1024, 1024))

    def rows_copy(kind, way, arriving):
        hops = (1 if kind < 2 else 2) if arriving else (0 if kind < 2 else 1)
        block = (x + 4 - hops) % 4 if way == 0 else (x + hops) % 4
        part = halves[1 - way] if kind == 1 else halves[way]
        piece = nbuf.at[block, :, part]
        return to_peer(way == 0, piece, piece, gs.at[0], gr.at[kind, way])

    for kind in (0, 1):
        for way in (0, 1):
            rows_copy(kind, way, False).start()
    for what in AFTER_SUM:
        if what == "relay":
            with jax.named_scope("relay"):
                for way in (0, 1):
                    rows_copy(0, way, True).wait_recv()
                    rows_copy(2, way, False).start()
        else:
            take(*what)
    with jax.named_scope("upwait"):
        for ev in range(16):
            wait_partner(UP, ev, partner_slot(*ORDER[ev]))
    with jax.named_scope("drainkv"):
        drain(KV)
    with jax.named_scope("rowswait"):
        for kind in (1, 2):
            for way in (0, 1):
                rows_copy(kind, way, True).wait_recv()

    def up(j, carry):
        cols = pl.ds(pl.multiple_of(j * 512, 512), 512)
        rows = nbuf[...].reshape(256, 2048)
        weights = wbuf[0, :, :, cols].reshape(2048, 512)
        part = jnp.maximum(jnp.dot(rows, weights, preferred_element_type=F32), 0.0)
        hidden[:, cols] = (part * part).astype(BF16)
        return carry

    with jax.named_scope("up"):
        lax.fori_loop(0, 2, up, 0)
    for what in AMID_UP:
        take(*what)
    with jax.named_scope("up"):
        lax.fori_loop(2, 4, up, 0)

    def chunk_sum(k):
        low_, high = CHUNKS[k]
        cols = pl.ds(low_ * 128, (high - low_) * 128)
        part = pl.ds(low_ * 64, (high - low_) * 64)
        return TpSum(k + 1, lambda r: dbuf.at[r, :, cols], lambda w: dhalf.at[w, :, part], lambda w: frecv.at[w, :, cols])

    sums = [chunk_sum(k) for k in range(len(CHUNKS))]

    last_cols = pl.ds(CHUNKS[-1][0] * 128, (CHUNKS[-1][1] - CHUNKS[-1][0]) * 128)

    def last_copy(d):
        return pltpu.make_async_remote_copy(
            src_ref=dbuf.at[(x + d) % 4, :, last_cols], dst_ref=lastbuf.at[d - 1], send_sem=xs.at[1], recv_sem=lr.at[d - 1],
            device_id=(sp, (x + d) % 4), device_id_type=MESH,
        )

    def last_total():
        total = dbuf[x, :, last_cols].astype(F32)
        for d in (1, 3, 2):
            last_copy(d).wait_recv()
            total = total + lastbuf[d - 1].astype(F32)
        return total

    def collect(k):
        total = last_total() if k == len(CHUNKS) - 1 else sums[k].total()
        places = ORDER[slice(*CHUNKS[k])]
        blocks = [slot(*place) for place in places] + [partner_slot(*place) for place in places]
        for b, block in enumerate(blocks):
            piece = total[:, (b // 2) * 128 : (b // 2) * 128 + 128]
            if b % 2 == 1:
                piece = pltpu.roll(piece, 64, 1)
            stage[block] = piece

    def down(k):
        first_, last_ = CHUNKS[k]
        places = ORDER[first_:last_]
        with jax.named_scope("dwait"):
            for r in range(first_, last_):
                wait_partner(DOWN, r, partner_slot(*ORDER[r]))
        blocks = [slot(*place) for place in places] + [partner_slot(*place) for place in places]
        part = nt_dot(hidden[...], jnp.concatenate([wbuf[1, b] for b in blocks], axis=0)).astype(BF16)
        for r in range(4):
            dbuf[r, :, first_ * 128 : last_ * 128] = part[r * 64 : (r + 1) * 64, :]
        if k == len(CHUNKS) - 1:
            for d in (2, 1, 3):
                last_copy(d).start()
        else:
            sums[k].start()

    for what in TAIL:
        if isinstance(what, tuple):
            take(*what)
        else:
            with jax.named_scope(what):
                kind, k = what[:-1], int(what[-1])
                if kind == "down":
                    down(k)
                elif kind == "combine":
                    sums[k].combine()
                else:
                    collect(k)
    drain(UP)
    drain(DOWN)
    drain_tp(pout, xs.at[0])
    drain_tp(nbuf, gs.at[0])
    with jax.named_scope("assemble"):
        for pos in range(16):
            both_halves = jnp.where(low, stage[2 * pos], pltpu.roll(stage[2 * pos + 1], 64, 1))
            cols = slice(pos * 128, pos * 128 + 128)
            out_ref[:, cols] = (midbuf[:, cols] + both_halves).astype(BF16)

    with jax.named_scope("draintp"):
        drain_tp(dbuf, xs.at[1])


def local(
    resid, query_a, key_a, value_a, query_b, key_b, value_b, gain_qa, gain_ka, gain_qb, gain_kb,
    w_out_a, w_out_b, norm_gain, w_up, w_down,
):
    rowtab, coltab = build_tables()
    vmem = pl.BlockSpec(memory_space=pltpu.VMEM)
    anywhere = pl.BlockSpec(memory_space=pl.ANY)
    dma = pltpu.SemaphoreType.DMA
    return pl.pallas_call(
        kernel,
        out_shape=pltpu.VMEM((64, 2048), BF16),
        in_specs=[vmem] * 13 + [anywhere] * 5,
        out_specs=vmem,
        scratch_shapes=[
            pltpu.VMEM((32, 768, 128), BF16),
            pltpu.VMEM((2, 32, 64, 2048), BF16),
            pltpu.VMEM((512, 2048), BF16),
            pltpu.VMEM((64, 2048), BF16),
            pltpu.VMEM((4, 128, 512), BF16),
            pltpu.VMEM((2, 128, 256), BF16),
            pltpu.VMEM((6, 512, 256), F32),
            pltpu.VMEM((6, 512, 256), F32),
            pltpu.VMEM((6, 8, 256), F32),
            pltpu.VMEM((4, 80, 256), F32),
            pltpu.VMEM((2, 144, 256), F32),
            pltpu.VMEM((256, 512), BF16),
            pltpu.VMEM((4, 64, 2048), BF16),
            pltpu.VMEM((2, 64, 1024), BF16),
            pltpu.VMEM((2, 64, 2048), BF16),
            pltpu.VMEM((4, 64, 2048), BF16),
            pltpu.VMEM((256, 2048), BF16),
            pltpu.VMEM((4, 64, 2048), BF16),
            pltpu.VMEM((2, 64, 1024), BF16),
            pltpu.VMEM((2, 64, 2048), BF16),
            pltpu.VMEM((32, 64, 128), F32),
            pltpu.VMEM((64, 2048), F32),
            pltpu.VMEM((3, 64, 256), BF16),
            dma((5,)),
            dma((3,)),
            dma((3, 16)),
            dma((3, 16)),
            dma((2,)),
            dma((5, 2, 2)),
            dma((1,)),
            dma((3, 2)),
            dma((3,)),
        ],
        compiler_params=pltpu.CompilerParams(
            collective_id=0, has_side_effects=True, vmem_limit_bytes=58 * 1024 * 1024
        ),
    )(
        query_a, key_a.T, value_a.T, query_b, key_b, value_b,
        gain_qa.reshape(1, -1), gain_ka.reshape(1, -1), gain_qb.reshape(1, -1), gain_kb.reshape(1, -1),
        norm_gain.reshape(1, -1), jnp.asarray(rowtab), jnp.asarray(coltab),
        resid, w_out_a, w_out_b, w_up, w_down.T,
    )


def solution(mesh):
    return jax.shard_map(
        local,
        mesh=mesh,
        in_specs=(
            P(("sp", "tp"), None),
            P("sp", "tp"),
            P("sp", "tp"),
            P("sp", "tp"),
            P("sp", "tp"),
            P("sp", "tp"),
            P("sp", "tp"),
            P(),
            P(),
            P(),
            P(),
            P("tp", None),
            P("tp", None),
            P(),
            P("sp", "tp"),
            P("tp", "sp"),
        ),
        out_specs=P(("sp", "tp"), None),
        check_vma=False,
    )
```

```python
import functools
import math

import jax
import jax.numpy as jnp
import numpy as np
from jax import lax
from jax.experimental import pallas as pl
from jax.experimental.pallas import tpu as pltpu
from jax.sharding import PartitionSpec as P

MESH = pl.DeviceIdType.MESH
EPS = 1e-06
F32 = jnp.float32
BF16 = jnp.bfloat16
LOG2E = 1.4426950408889634
KV, UP, DOWN = 0, 1, 2
ORDER = (
    (0, 0), (3, 0), (1, 0), (0, 3), (0, 1), (2, 0), (3, 3), (3, 1),
    (1, 3), (1, 1), (0, 2), (2, 3), (2, 1), (3, 2), (1, 2), (2, 2),
)


def build_tables():
    rows, cols = [], []
    for width in (64, 128):
        quarter = width // 4
        freqs = (10000.0 ** (-(2.0 * np.arange(quarter)) / (width // 2))).astype(np.float32)
        freqs = np.concatenate([freqs, freqs])
        entry = np.arange(width)
        sign = np.where((entry // quarter) % 2 == 0, -1.0, 1.0)

        def pair(count, low):
            ang = (np.arange(count, dtype=np.float32)[:, None] * freqs).astype(np.float64)
            full = np.zeros((2, count, width))
            half = slice(0, width // 2) if low else slice(width // 2, width)
            full[0][:, half] = np.cos(ang)
            full[1][:, half] = np.sin(ang)
            full[1] *= sign
            return np.tile(full, (1, 1, 128 // width)).astype(np.float32)

        rows.append(pair(128, True))
        cols.append(pair(64, False))
    row = np.concatenate(rows, axis=0)
    row = row.reshape(4, 32, 4, 128).transpose(1, 0, 2, 3).reshape(32, 16, 128)
    col = np.concatenate(cols, axis=0)
    return row, col


def nt_dot(a, b):
    return lax.dot_general(a, b, (((1,), (1,)), ((), ())), preferred_element_type=F32)


def nn_dot(a, b):
    return jnp.dot(a, b, preferred_element_type=F32)


def pick(i, values):
    result = jnp.int32(values[0])
    for number, value in enumerate(values[1:]):
        result = jnp.where(i == number + 1, jnp.int32(value), result)
    return result


PLAN = {
    1: [(0, 1), (0, 2), (0, 3), (0, 4)],
    4: [(0, 5)],
    5: [(0, 6), (0, 7)],
    7: [(0, 8), (0, 9)],
    8: [(0, 10)],
    10: [(0, 11), (0, 12)],
    11: [(0, 13), (1, "b")],
    12: [(0, 14)],
    14: [(0, 15), (1, 1), (1, 2)],
    15: [],
    16: [(1, 3), (1, 4)],
}
AFTER_PROJECT = [(1, 5), (1, 6), (1, 7), (2, "a"), (2, "b"), "combine", (1, 8), (1, 9), (1, 10)]
AFTER_SUM = [(1, 11), (1, 12), (2, 1), (2, 2), (1, 13), "relay", (1, 14), (2, 5), (2, 3), (2, 4), (1, 15)]
AMID_UP = [(2, 6), (2, 7)]
CHUNKS = ((0, 4), (4, 8), (8, 12), (12, 14), (14, 16))
TAIL = [
    "down0", (2, 8), (2, 9), "down1", (2, 11), (2, 12), "combine0", (2, 10), "down2", (2, 13), (2, 14), "combine1", "collect0",
    "down3", (2, 15), "combine2", "down4", "collect1", "combine3", "collect2", "collect3", "collect4",
]


def kernel(
    ka_hbm, va_hbm, kb_hbm, vb_hbm, gka_hbm, gkb_hbm, rowtab_hbm, coltab_hbm,
    qa_hbm, qb_hbm, gqa_hbm, gqb_hbm, ngain_hbm,
    resid_hbm, woa_hbm, wob_hbm, wup_hbm, wdown_hbm,
    out_ref,
    ka_ref, va_ref, kb_ref, vb_ref, gka_ref, gkb_ref, rowtab_ref, coltab_ref,
    qa_ref, qb_ref, gqa_ref, gqb_ref, ngain_ref,
    kvbuf, wbuf, wo, resid, qa, qb, s_even, s_odd, tops, acc_a, acc_b, attn,
    pout, phalf, rsbuf, nbuf, hidden, dbuf, dhalf, frecv, stage, midbuf, lastbuf,
    lsem, ssem, rsem, precv, xs, xr, gs, gr, lr,
):
    sp = lax.axis_index("sp")
    x = lax.axis_index("tp")
    z, y, c = sp // 8, (sp // 2) % 4, sp % 2
    n = 1 - c
    partner = z * 8 + y * 2 + n

    def slot(da, db):
        return ((z + n * db + c * da) % 4) * 8 + ((y + n * da + c * db) % 4) * 2 + c

    def partner_slot(da, db):
        return ((z + c * db + n * da) % 4) * 8 + ((y + c * da + n * db) % 4) * 2 + n

    def event(da, db):
        return ORDER.index((da, db))

    barrier = pltpu.get_barrier_semaphore()
    others = [(slot(1, 0), x), (slot(3, 0), x), (slot(0, 1), x), (slot(0, 3), x), (partner, x)]
    others += [(sp, (x + d) % 4) for d in (1, 2, 3)]
    for dev in others:
        pl.semaphore_signal(barrier, inc=1, device_id=dev, device_id_type=MESH)

    loads = [
        pltpu.make_async_copy(wup_hbm, wbuf.at[0, sp], lsem.at[0]),
        pltpu.make_async_copy(wdown_hbm, wbuf.at[1, sp], lsem.at[1]),
        pltpu.make_async_copy(woa_hbm, wo.at[pl.ds(0, 256)], lsem.at[2]),
        pltpu.make_async_copy(wob_hbm, wo.at[pl.ds(256, 256)], lsem.at[3]),
        pltpu.make_async_copy(resid_hbm, resid, lsem.at[4]),
    ]
    pairs = [
        (ka_hbm, ka_ref), (va_hbm, va_ref), (kb_hbm, kb_ref), (vb_hbm, vb_ref), (gka_hbm, gka_ref), (gkb_hbm, gkb_ref),
        (rowtab_hbm.at[sp], rowtab_ref), (coltab_hbm, coltab_ref),
        (qa_hbm, qa_ref), (qb_hbm, qb_ref), (gqa_hbm, gqa_ref), (gqb_hbm, gqb_ref), (ngain_hbm, ngain_ref),
    ]
    inputs = [pltpu.make_async_copy(src, dst, lsem.at[5 + number]) for number, (src, dst) in enumerate(pairs)]
    for load in inputs + loads:
        load.start()

    def region(item, index, half):
        if item == KV:
            ref, size = kvbuf.at[index], 384
        else:
            ref, size = wbuf.at[item - 1, index], 32
        if half is None:
            return ref
        return ref.at[pl.ds(half * size, size)]

    def block_copy(item, piece, recv_sem, to):
        return pltpu.make_async_remote_copy(
            src_ref=piece, dst_ref=piece, send_sem=ssem.at[item], recv_sem=recv_sem, device_id=(to, x), device_id_type=MESH,
        )

    def send(item, index, half, to, there):
        block_copy(item, region(item, index, half), rsem.at[item, event(*there)], slot(*to)).start()

    def hand_over(item, ev, index):
        block_copy(item, region(item, index, None), precv.at[item, ev], partner).start()

    def wait_in(item, ev, index):
        block_copy(item, region(item, index, None), rsem.at[item, ev], partner).wait_recv()

    def wait_partner(item, ev, index):
        block_copy(item, region(item, index, None), precv.at[item, ev], partner).wait_recv()

    def drain(item):
        ref = kvbuf.at[pl.ds(0, 31)] if item == KV else wbuf.at[item - 1, pl.ds(0, 31)]
        block_copy(item, ref, rsem.at[item, 0], partner).wait_send()

    def take(item, number):
        with jax.named_scope(f"take{item}_{number}"):
            if number in ("a", "b"):
                start_own(item, number)
            else:
                take_in(item, *ORDER[number])

    def start_own(item, ring):
        index = slot(0, 0)
        if ring == "a":
            send(item, index, None, (1, 0), (3, 0))
            send(item, index, None, (3, 0), (1, 0))
        else:
            send(item, index, None, (0, 1), (0, 3))
            send(item, index, None, (0, 3), (0, 1))
            hand_over(item, 0, index)

    def take_in(item, da, db):
        ev, index = event(da, db), slot(da, db)
        wait_in(item, ev, index)
        if db == 0:
            if da == 3:
                send(item, index, 0, (1, 0), (2, 0))
            elif da == 1:
                send(item, index, 1, (3, 0), (2, 0))
            send(item, index, None, (0, 1), (da, 3))
            send(item, index, None, (0, 3), (da, 1))
        elif db == 3:
            send(item, index, 0, (0, 1), (da, 2))
        elif db == 1:
            send(item, index, 1, (0, 3), (da, 2))
        hand_over(item, ev, index)

    def own_up(half):
        part = pl.ds(half * 32, 32)
        for to, there in (((1, 0), (3, 0)), ((3, 0), (1, 0))):
            pltpu.make_async_remote_copy(
                src_ref=wup_hbm.at[part], dst_ref=wbuf.at[0, sp, part], send_sem=ssem.at[UP], recv_sem=rsem.at[UP, event(*there)],
                device_id=(slot(*to), x), device_id_type=MESH,
            ).start()

    with jax.named_scope("barrier"):
        pl.semaphore_wait(barrier, len(others))
    own_up(0)

    with jax.named_scope("inputs"):
        for load in inputs[0:8]:
            load.wait()
    lane = lax.broadcasted_iota(jnp.int32, (64, 128), 1)
    low = lane < 64
    rowtab = rowtab_ref[...]

    def both_heads(ref):
        return jnp.concatenate([ref[...], ref[...]], axis=1)

    def rotate(v, gain, width, r, s):
        quarter = width // 4
        kind = 0 if width == 64 else 2

        def angles(which):
            across = rowtab[which * 4 + r : which * 4 + r + 1]
            if s != r:
                across = jnp.where(low[0:1], across, rowtab[which * 4 + s : which * 4 + s + 1])
            return across + coltab_ref[which]

        sq = v * v
        if width == 64:
            left = jnp.sum(jnp.where(low, sq, 0.0), axis=-1, keepdims=True)
            right = jnp.sum(jnp.where(low, 0.0, sq), axis=-1, keepdims=True)
            mean = jnp.where(low, left, right) * (1.0 / 64)
        else:
            mean = jnp.sum(sq, axis=-1, keepdims=True) * (1.0 / 128)
        u = v * lax.rsqrt(mean + EPS) * gain
        even = (lane // quarter) % 2 == 0
        turned = jnp.where(even, pltpu.roll(u, 128 - quarter, 1), pltpu.roll(u, quarter, 1))
        return u * angles(kind) + turned * angles(kind + 1)

    own = slot(0, 0)
    turned = ka_ref[...].astype(F32)
    turned = jnp.concatenate([turned[:, 0:128], turned[:, 128:256]], axis=0).T
    gain = both_heads(gka_ref)
    for r in range(2):
        block = rotate(turned[r * 64 : (r + 1) * 64], gain, 64, r, r + 2)
        kvbuf[own, r * 64 : (r + 1) * 64, :] = block.astype(BF16)
    for r in range(4):
        block = rotate(kb_ref[r * 64 : (r + 1) * 64, :].astype(F32), gkb_ref[...], 128, r, r)
        kvbuf[own, 128 + r * 64 : 192 + r * 64, :] = block.astype(BF16)
    for half in range(2):
        tokens = slice(half * 128, half * 128 + 128)
        kvbuf[own, 384 + half * 64 : 448 + half * 64, :] = va_ref[:, tokens]
        kvbuf[own, 512 + half * 128 : 640 + half * 128, :] = vb_ref[tokens, :].astype(F32).T.astype(BF16)

    take(KV, "a")
    take(KV, "b")
    loads[0].wait()
    own_up(1)

    with jax.named_scope("queries"):
        for load in inputs[8:]:
            load.wait()
        gain_a = both_heads(gqa_ref)
        for g in range(2):
            lanes = slice(g * 128, g * 128 + 128)
            rows = [slice(r * 64, r * 64 + 64) for r in range(4)]
            heads = [rotate(qa_ref[rows[r], lanes].astype(F32), gain_a, 64, r, r) for r in range(4)]
            heads = jnp.concatenate(heads, axis=0).T.astype(BF16)
            for h in range(2):
                head = heads[h * 64 : h * 64 + 64]
                qa[2 * g + h, 0:64, 0:256] = head
                qa[2 * g + h, 0:64, 256:512] = jnp.zeros_like(head)
                qa[2 * g + h, 64:128, 0:256] = jnp.zeros_like(head)
                qa[2 * g + h, 64:128, 256:512] = head
            heads = [rotate(qb_ref[rows[r], lanes].astype(F32), gqb_ref[...], 128, r, r) for r in range(4)]
            qb[g] = jnp.concatenate(heads, axis=0).T.astype(BF16)
        tops[...] = jnp.full_like(tops, -1e30)
        acc_a[...] = jnp.zeros_like(acc_a)
        acc_b[...] = jnp.zeros_like(acc_b)

    scale_a = 64 ** (-0.5) * LOG2E
    scale_b = 128 ** (-0.5) * LOG2E

    def turned_values(pieces):
        values = jnp.concatenate(pieces, axis=1)
        return jnp.concatenate([values, jnp.ones((16, 512), BF16)], axis=0)

    def score(pair, target):
        keys_a = jnp.concatenate([kvbuf[s, 0:128, :] for s in pair], axis=0)
        keys_b = jnp.concatenate([kvbuf[s, 128:384, :] for s in pair], axis=0)

        def one(h):
            if h < 4:
                scores = nn_dot(keys_a, qa[h]) * scale_a
                scores = jnp.concatenate([scores[:, 0:256], scores[:, 256:512]], axis=0)
            else:
                scores = nn_dot(keys_b, qb[h - 4]) * scale_b
            target[h] = scores
            before = tops[h, 0:1, :]
            top = jnp.maximum(before, jnp.max(scores, axis=0, keepdims=True))
            tops[h, 0:1, :] = top
            tops[h, 1:2, :] = jnp.exp2(before - top)

        return one

    def gather_values(pair):
        def one(h):
            if h < 4:
                return turned_values([kvbuf[s, 384 + 64 * half : 448 + 64 * half, :] for half in range(2) for s in pair])
            return turned_values([kvbuf[s, 512 + 128 * half : 640 + 128 * half, :] for s in pair for half in range(2)])

        return one(0), one(4)

    def use(source, h, values, top, factor):
        expo = jnp.exp2(source[h] - top).astype(BF16)
        got = nn_dot(values[0] if h < 4 else values[1], expo)
        acc, index = (acc_a, h) if h < 4 else (acc_b, h - 4)
        acc[index] = acc[index] * factor + got

    def both(now, after, source, target):
        values = gather_values(now)
        scorer = None if after is None else score(after, target)
        for h in range(6):
            top, factor = tops[h, 0:1, :], tops[h, 1:2, :]
            if scorer is not None:
                scorer(h)
            use(source, h, values, top, factor)

    def my_block(t, shift):
        places = ORDER[shift::2]
        return slot(pick(t, [p[0] for p in places]), pick(t, [p[1] for p in places]))

    def partner_block(t, shift):
        places = ORDER[shift::2]
        return partner_slot(pick(t, [p[0] for p in places]), pick(t, [p[1] for p in places]))

    def ready(t, shift):
        for number in range(6):
            if PLAN.get(2 * number + shift):

                @pl.when(t == number)
                def _(number=number):
                    for what in PLAN[2 * number + shift]:
                        take(*what)

    def fetch(number, t, shift):
        theirs = partner_block(t, shift - 1)
        with jax.named_scope("pwait"):
            wait_partner(KV, number - 1, theirs)
        return my_block(t, shift + 1), theirs

    def attend(t, pair):
        with jax.named_scope("step"):
            ready(t, 2)
            middle = fetch(2 * t + 2, t, 2)
            both(pair, middle, s_odd, s_even)
            ready(t, 3)
            after = fetch(2 * t + 3, t, 3)
            both(middle, after, s_even, s_odd)
        return after

    loads[1].wait()
    with jax.named_scope("first"):
        wait_partner(KV, 0, partner)
        pair = (own, partner)
        first = score(pair, s_even)
        for h in range(6):
            first(h)
        for what in PLAN[1]:
            take(*what)
        after = (slot(*ORDER[1]), slot(*ORDER[2]))
        both(pair, after, s_even, s_odd)
    pair = lax.fori_loop(0, 6, attend, after)
    with jax.named_scope("laststep"):
        for what in PLAN[14]:
            take(*what)
        theirs = partner_slot(*ORDER[13])
        wait_partner(KV, 13, theirs)
        middle = (slot(*ORDER[15]), theirs)
        both(pair, middle, s_odd, s_even)
        for what in PLAN[15]:
            take(*what)
        after = (partner_slot(*ORDER[14]), partner_slot(*ORDER[15]))
        wait_partner(KV, 14, after[0])
        wait_partner(KV, 15, after[1])
        both(middle, after, s_even, s_odd)
        both(after, None, s_odd, None)
        for what in PLAN[16]:
            take(*what)

    for h in range(4):
        acc = acc_a[h]
        acc_a[h, 0:64, :] = acc[0:64] / acc[64:65]
    for g in range(2):
        both_rows = jnp.concatenate([acc_a[2 * g, 0:64, :], acc_a[2 * g + 1, 0:64, :]], axis=0)
        attn[:, g * 128 : (g + 1) * 128] = both_rows.T.astype(BF16)
        acc = acc_b[g]
        attn[:, 256 + g * 128 : 256 + (g + 1) * 128] = (acc[0:128] / acc[128:129]).T.astype(BF16)
    loads[2].wait()
    loads[3].wait()

    def project(j, carry):
        cols = pl.ds(pl.multiple_of(j * 512, 512), 512)
        part = jnp.dot(attn[...], wo[:, cols], preferred_element_type=F32).astype(BF16)
        for r in range(4):
            pout[r, :, cols] = part[r * 64 : (r + 1) * 64, :]
        return carry

    with jax.named_scope("project"):
        lax.fori_loop(0, 4, project, 0)

    def to_peer(forward, src, dst, send_sem, recv_sem):
        return pltpu.make_async_remote_copy(
            src_ref=src,
            dst_ref=dst,
            send_sem=send_sem,
            recv_sem=recv_sem,
            device_id=(sp, (x + (1 if forward else 3)) % 4),
            device_id_type=MESH,
        )

    class TpSum:
        def __init__(self, number, blocks, halves, received):
            self.number, self.blocks, self.halves, self.received = number, blocks, halves, received
            width = received(0).shape[1] // 2
            self.parts = (pl.ds(0, width), pl.ds(width, width))

        def copy(self, kind, way):
            near = self.blocks((x + (1, 3)[way]) % 4)
            if kind == 0:
                src, dst = self.blocks((x + 2) % 4).at[:, self.parts[way]], self.halves(way)
            else:
                part = self.parts[1 - way] if kind == 1 else self.parts[way]
                src, dst = near.at[:, part], self.received(way).at[:, part]
            return to_peer(way == 0, src, dst, xs.at[min(self.number, 1)], xr.at[self.number, min(kind, 1), way])

        def start(self):
            for kind in (0, 1):
                for way in (0, 1):
                    self.copy(kind, way).start()

        def combine(self):
            for way in (0, 1):
                self.copy(0, way).wait_recv()
                near, part = self.blocks((x + (1, 3)[way]) % 4), self.parts[way]
                near[:, part] = (near[:, part].astype(F32) + self.halves(way)[...].astype(F32)).astype(BF16)
                self.copy(2, way).start()

        def total(self):
            for way in (0, 1):
                block = self.received(way)
                to_peer(True, block, block, xs.at[0], xr.at[self.number, 1, way]).wait_recv()
            return self.blocks(x)[...].astype(F32) + self.received(0)[...].astype(F32) + self.received(1)[...].astype(F32)

    def drain_tp(ref, sem):
        three = ref.at[pl.ds(0, 3)]
        to_peer(True, three, three, sem, xr.at[0, 0, 0]).wait_send()

    proj = TpSum(0, lambda r: pout.at[r], lambda w: phalf.at[w], lambda w: rsbuf.at[w])
    proj.start()
    for what in AFTER_PROJECT:
        if what == "combine":
            with jax.named_scope("combine"):
                proj.combine()
        else:
            take(*what)
    loads[4].wait()
    with jax.named_scope("rswait"):
        total = proj.total()
    mid = (resid[...].astype(F32) + total).astype(BF16).astype(F32)
    midbuf[...] = mid
    norm = mid * lax.rsqrt(jnp.mean(mid * mid, axis=-1, keepdims=True) + EPS) * ngain_ref[...]
    nbuf[x] = norm.astype(BF16)

    halves = (pl.ds(0, 1024), pl.ds(1024, 1024))

    def rows_copy(kind, way, arriving):
        hops = (1 if kind < 2 else 2) if arriving else (0 if kind < 2 else 1)
        block = (x + 4 - hops) % 4 if way == 0 else (x + hops) % 4
        part = halves[1 - way] if kind == 1 else halves[way]
        piece = nbuf.at[block, :, part]
        return to_peer(way == 0, piece, piece, gs.at[0], gr.at[kind, way])

    for kind in (0, 1):
        for way in (0, 1):
            rows_copy(kind, way, False).start()
    for what in AFTER_SUM:
        if what == "relay":
            with jax.named_scope("relay"):
                for way in (0, 1):
                    rows_copy(0, way, True).wait_recv()
                    rows_copy(2, way, False).start()
        else:
            take(*what)
    with jax.named_scope("upwait"):
        for ev in range(16):
            wait_partner(UP, ev, partner_slot(*ORDER[ev]))
    with jax.named_scope("drainkv"):
        drain(KV)
    with jax.named_scope("rowswait"):
        for kind in (1, 2):
            for way in (0, 1):
                rows_copy(kind, way, True).wait_recv()

    def up(j, carry):
        cols = pl.ds(pl.multiple_of(j * 512, 512), 512)
        rows = nbuf[...].reshape(256, 2048)
        weights = wbuf[0, :, :, cols].reshape(2048, 512)
        part = jnp.maximum(jnp.dot(rows, weights, preferred_element_type=F32), 0.0)
        hidden[:, cols] = (part * part).astype(BF16)
        return carry

    with jax.named_scope("up"):
        lax.fori_loop(0, 2, up, 0)
    for what in AMID_UP:
        take(*what)
    with jax.named_scope("up"):
        lax.fori_loop(2, 4, up, 0)

    def chunk_sum(k):
        low_, high = CHUNKS[k]
        cols = pl.ds(low_ * 128, (high - low_) * 128)
        part = pl.ds(low_ * 64, (high - low_) * 64)
        return TpSum(k + 1, lambda r: dbuf.at[r, :, cols], lambda w: dhalf.at[w, :, part], lambda w: frecv.at[w, :, cols])

    sums = [chunk_sum(k) for k in range(len(CHUNKS))]

    last_cols = pl.ds(CHUNKS[-1][0] * 128, (CHUNKS[-1][1] - CHUNKS[-1][0]) * 128)

    def last_copy(d):
        return pltpu.make_async_remote_copy(
            src_ref=dbuf.at[(x + d) % 4, :, last_cols], dst_ref=lastbuf.at[d - 1], send_sem=xs.at[1], recv_sem=lr.at[d - 1],
            device_id=(sp, (x + d) % 4), device_id_type=MESH,
        )

    def last_total():
        total = dbuf[x, :, last_cols].astype(F32)
        for d in (1, 3, 2):
            last_copy(d).wait_recv()
            total = total + lastbuf[d - 1].astype(F32)
        return total

    def collect(k):
        total = last_total() if k == len(CHUNKS) - 1 else sums[k].total()
        places = ORDER[slice(*CHUNKS[k])]
        blocks = [slot(*place) for place in places] + [partner_slot(*place) for place in places]
        for b, block in enumerate(blocks):
            piece = total[:, (b // 2) * 128 : (b // 2) * 128 + 128]
            if b % 2 == 1:
                piece = pltpu.roll(piece, 64, 1)
            stage[block] = piece

    def down(k):
        first_, last_ = CHUNKS[k]
        places = ORDER[first_:last_]
        with jax.named_scope("dwait"):
            for r in range(first_, last_):
                wait_partner(DOWN, r, partner_slot(*ORDER[r]))
        blocks = [slot(*place) for place in places] + [partner_slot(*place) for place in places]
        part = nt_dot(hidden[...], jnp.concatenate([wbuf[1, b] for b in blocks], axis=0)).astype(BF16)
        for r in range(4):
            dbuf[r, :, first_ * 128 : last_ * 128] = part[r * 64 : (r + 1) * 64, :]
        if k == len(CHUNKS) - 1:
            for d in (2, 1, 3):
                last_copy(d).start()
        else:
            sums[k].start()

    for what in TAIL:
        if isinstance(what, tuple):
            take(*what)
        else:
            with jax.named_scope(what):
                kind, k = what[:-1], int(what[-1])
                if kind == "down":
                    down(k)
                elif kind == "combine":
                    sums[k].combine()
                else:
                    collect(k)
    drain(UP)
    drain(DOWN)
    drain_tp(pout, xs.at[0])
    drain_tp(nbuf, gs.at[0])
    with jax.named_scope("assemble"):
        for pos in range(16):
            both_halves = jnp.where(low, stage[2 * pos], pltpu.roll(stage[2 * pos + 1], 64, 1))
            cols = slice(pos * 128, pos * 128 + 128)
            out_ref[:, cols] = (midbuf[:, cols] + both_halves).astype(BF16)

    with jax.named_scope("draintp"):
        drain_tp(dbuf, xs.at[1])


def local(
    resid, query_a, key_a, value_a, query_b, key_b, value_b, gain_qa, gain_ka, gain_qb, gain_kb,
    w_out_a, w_out_b, norm_gain, w_up, w_down,
):
    rowtab, coltab = build_tables()
    vmem = pl.BlockSpec(memory_space=pltpu.VMEM)
    anywhere = pl.BlockSpec(memory_space=pl.ANY)
    dma = pltpu.SemaphoreType.DMA
    return pl.pallas_call(
        kernel,
        out_shape=pltpu.VMEM((64, 2048), BF16),
        in_specs=[anywhere] * 18,
        out_specs=vmem,
        scratch_shapes=[
            pltpu.VMEM((64, 256), BF16),
            pltpu.VMEM((64, 256), BF16),
            pltpu.VMEM((256, 128), BF16),
            pltpu.VMEM((256, 128), BF16),
            pltpu.VMEM((1, 64), F32),
            pltpu.VMEM((1, 128), F32),
            pltpu.VMEM((16, 128), F32),
            pltpu.VMEM((4, 64, 128), F32),
            pltpu.VMEM((256, 256), BF16),
            pltpu.VMEM((256, 256), BF16),
            pltpu.VMEM((1, 64), F32),
            pltpu.VMEM((1, 128), F32),
            pltpu.VMEM((1, 2048), F32),
            pltpu.VMEM((32, 768, 128), BF16),
            pltpu.VMEM((2, 32, 64, 2048), BF16),
            pltpu.VMEM((512, 2048), BF16),
            pltpu.VMEM((64, 2048), BF16),
            pltpu.VMEM((4, 128, 512), BF16),
            pltpu.VMEM((2, 128, 256), BF16),
            pltpu.VMEM((6, 512, 256), F32),
            pltpu.VMEM((6, 512, 256), F32),
            pltpu.VMEM((6, 8, 256), F32),
            pltpu.VMEM((4, 80, 256), F32),
            pltpu.VMEM((2, 144, 256), F32),
            pltpu.VMEM((256, 512), BF16),
            pltpu.VMEM((4, 64, 2048), BF16),
            pltpu.VMEM((2, 64, 1024), BF16),
            pltpu.VMEM((2, 64, 2048), BF16),
            pltpu.VMEM((4, 64, 2048), BF16),
            pltpu.VMEM((256, 2048), BF16),
            pltpu.VMEM((4, 64, 2048), BF16),
            pltpu.VMEM((2, 64, 1024), BF16),
            pltpu.VMEM((2, 64, 2048), BF16),
            pltpu.VMEM((32, 64, 128), F32),
            pltpu.VMEM((64, 2048), F32),
            pltpu.VMEM((3, 64, 256), BF16),
            dma((18,)),
            dma((3,)),
            dma((3, 16)),
            dma((3, 16)),
            dma((2,)),
            dma((5, 2, 2)),
            dma((1,)),
            dma((3, 2)),
            dma((3,)),
        ],
        compiler_params=pltpu.CompilerParams(
            collective_id=0, has_side_effects=True, vmem_limit_bytes=58 * 1024 * 1024
        ),
    )(
        key_a.T, value_a.T, key_b, value_b, gain_ka.reshape(1, -1), gain_kb.reshape(1, -1),
        jnp.asarray(rowtab), jnp.asarray(coltab),
        query_a, query_b, gain_qa.reshape(1, -1), gain_qb.reshape(1, -1), norm_gain.reshape(1, -1),
        resid, w_out_a, w_out_b, w_up, w_down.T,
    )


def solution(mesh):
    return jax.shard_map(
        local,
        mesh=mesh,
        in_specs=(
            P(("sp", "tp"), None),
            P("sp", "tp"),
            P("sp", "tp"),
            P("sp", "tp"),
            P("sp", "tp"),
            P("sp", "tp"),
            P("sp", "tp"),
            P(),
            P(),
            P(),
            P(),
            P("tp", None),
            P("tp", None),
            P(),
            P("sp", "tp"),
            P("tp", "sp"),
        ),
        out_specs=P(("sp", "tp"), None),
        check_vma=False,
    )
```

```python
import functools
import math

import jax
import jax.numpy as jnp
import numpy as np
from jax import lax
from jax.experimental import pallas as pl
from jax.experimental.pallas import tpu as pltpu
from jax.sharding import PartitionSpec as P

MESH = pl.DeviceIdType.MESH
EPS = 1e-06
F32 = jnp.float32
BF16 = jnp.bfloat16
LOG2E = 1.4426950408889634
KV, UP, DOWN = 0, 1, 2
ORDER = (
    (0, 0), (3, 0), (1, 0), (0, 3), (0, 1), (2, 0), (3, 3), (3, 1),
    (1, 3), (1, 1), (0, 2), (2, 3), (2, 1), (3, 2), (1, 2), (2, 2),
)


def build_tables():
    rows, cols = [], []
    for width in (64, 128):
        quarter = width // 4
        freqs = (10000.0 ** (-(2.0 * np.arange(quarter)) / (width // 2))).astype(np.float32)
        freqs = np.concatenate([freqs, freqs])
        entry = np.arange(width)
        sign = np.where((entry // quarter) % 2 == 0, -1.0, 1.0)

        def pair(count, low):
            ang = (np.arange(count, dtype=np.float32)[:, None] * freqs).astype(np.float64)
            full = np.zeros((2, count, width))
            half = slice(0, width // 2) if low else slice(width // 2, width)
            full[0][:, half] = np.cos(ang)
            full[1][:, half] = np.sin(ang)
            full[1] *= sign
            return np.tile(full, (1, 1, 128 // width)).astype(np.float32)

        rows.append(pair(128, True))
        cols.append(pair(64, False))
    row = np.concatenate(rows, axis=0)
    row = row.reshape(4, 32, 4, 128).transpose(1, 0, 2, 3).reshape(32, 16, 128)
    col = np.concatenate(cols, axis=0)
    return row, col


def nt_dot(a, b):
    return lax.dot_general(a, b, (((1,), (1,)), ((), ())), preferred_element_type=F32)


def nn_dot(a, b):
    return jnp.dot(a, b, preferred_element_type=F32)


def pick(i, values):
    result = jnp.int32(values[0])
    for number, value in enumerate(values[1:]):
        result = jnp.where(i == number + 1, jnp.int32(value), result)
    return result


PLAN = {
    1: [(0, 1), (0, 2), (0, 3), (0, 4)],
    4: [(0, 5)],
    5: [(0, 6), (0, 7)],
    7: [(0, 8), (0, 9)],
    8: [(0, 10)],
    10: [(0, 11), (0, 12)],
    11: [(0, 13), (1, "b")],
    12: [(0, 14)],
    14: [(0, 15), (1, 1), (1, 2)],
    15: [],
    16: [(1, 3), (1, 4)],
}
AFTER_PROJECT = [(1, 5), (1, 6), (1, 7), (2, "a"), (2, "b"), "combine", (1, 8), (1, 9), (1, 10)]
AFTER_SUM = [(1, 11), (1, 12), (2, 1), (2, 2), (1, 13), "relay", (1, 14), (2, 5), (2, 3), (2, 4), (1, 15)]
AMID_UP = [(2, 6), (2, 7)]
CHUNKS = ((0, 4), (4, 8), (8, 12), (12, 14), (14, 16))
TAIL = [
    "down0", (2, 8), (2, 9), "down1", (2, 11), (2, 12), "combine0", (2, 10), "down2", (2, 13), (2, 14), "combine1", "collect0",
    "down3", (2, 15), "combine2", "down4", "collect1", "combine3", "collect2", "collect3", "collect4",
]


def kernel(
    ka_hbm, va_hbm, kb_hbm, vb_hbm, gka_hbm, gkb_hbm, rowtab_hbm, coltab_hbm,
    qa_hbm, qb_hbm, gqa_hbm, gqb_hbm, ngain_hbm,
    resid_hbm, woa_hbm, wob_hbm, wup_hbm, wdown_hbm,
    out_ref,
    ka_ref, va_ref, kb_ref, vb_ref, gka_ref, gkb_ref, rowtab_ref, coltab_ref,
    qa_ref, qb_ref, gqa_ref, gqb_ref, ngain_ref,
    kvbuf, wbuf, wo, resid, qa, qb, s_even, s_odd, tops, acc_a, acc_b, attn,
    pout, phalf, rsbuf, nbuf, hidden, dbuf, dhalf, frecv, stage, midbuf, lastbuf,
    lsem, ssem, rsem, precv, xs, xr, gs, gr, lr,
):
    sp = lax.axis_index("sp")
    x = lax.axis_index("tp")
    z, y, c = sp // 8, (sp // 2) % 4, sp % 2
    n = 1 - c
    partner = z * 8 + y * 2 + n

    def slot(da, db):
        return ((z + n * db + c * da) % 4) * 8 + ((y + n * da + c * db) % 4) * 2 + c

    def partner_slot(da, db):
        return ((z + c * db + n * da) % 4) * 8 + ((y + c * da + n * db) % 4) * 2 + n

    def event(da, db):
        return ORDER.index((da, db))

    barrier = pltpu.get_barrier_semaphore()
    others = [(slot(1, 0), x), (slot(3, 0), x), (slot(0, 1), x), (slot(0, 3), x), (partner, x)]
    others += [(sp, (x + d) % 4) for d in (1, 2, 3)]
    for dev in others:
        pl.semaphore_signal(barrier, inc=1, device_id=dev, device_id_type=MESH)

    loads = [
        pltpu.make_async_copy(wup_hbm, wbuf.at[0, sp], lsem.at[0]),
        pltpu.make_async_copy(wdown_hbm, wbuf.at[1, sp], lsem.at[1]),
        pltpu.make_async_copy(woa_hbm, wo.at[pl.ds(0, 256)], lsem.at[2]),
        pltpu.make_async_copy(wob_hbm, wo.at[pl.ds(256, 256)], lsem.at[3]),
        pltpu.make_async_copy(resid_hbm, resid, lsem.at[4]),
    ]
    pairs = [
        (ka_hbm, ka_ref), (va_hbm, va_ref), (kb_hbm, kb_ref), (vb_hbm, vb_ref), (gka_hbm, gka_ref), (gkb_hbm, gkb_ref),
        (rowtab_hbm.at[sp], rowtab_ref), (coltab_hbm, coltab_ref),
        (qa_hbm, qa_ref), (qb_hbm, qb_ref), (gqa_hbm, gqa_ref), (gqb_hbm, gqb_ref), (ngain_hbm, ngain_ref),
    ]
    inputs = [pltpu.make_async_copy(src, dst, lsem.at[5 + number]) for number, (src, dst) in enumerate(pairs)]
    for load in inputs + loads:
        load.start()

    def region(item, index, half):
        if item == KV:
            ref, size = kvbuf.at[index], 384
        else:
            ref, size = wbuf.at[item - 1, index], 32
        if half is None:
            return ref
        return ref.at[pl.ds(half * size, size)]

    def block_copy(item, piece, recv_sem, to):
        return pltpu.make_async_remote_copy(
            src_ref=piece, dst_ref=piece, send_sem=ssem.at[item], recv_sem=recv_sem, device_id=(to, x), device_id_type=MESH,
        )

    def send(item, index, half, to, there):
        block_copy(item, region(item, index, half), rsem.at[item, event(*there)], slot(*to)).start()

    def hand_over(item, ev, index):
        block_copy(item, region(item, index, None), precv.at[item, ev], partner).start()

    def wait_in(item, ev, index):
        block_copy(item, region(item, index, None), rsem.at[item, ev], partner).wait_recv()

    def wait_partner(item, ev, index):
        block_copy(item, region(item, index, None), precv.at[item, ev], partner).wait_recv()

    def drain(item):
        ref = kvbuf.at[pl.ds(0, 31)] if item == KV else wbuf.at[item - 1, pl.ds(0, 31)]
        block_copy(item, ref, rsem.at[item, 0], partner).wait_send()

    def take(item, number):
        with jax.named_scope(f"take{item}_{number}"):
            if number in ("a", "b"):
                start_own(item, number)
            else:
                take_in(item, *ORDER[number])

    def start_own(item, ring):
        index = slot(0, 0)
        if ring == "a":
            send(item, index, None, (1, 0), (3, 0))
            send(item, index, None, (3, 0), (1, 0))
        else:
            send(item, index, None, (0, 1), (0, 3))
            send(item, index, None, (0, 3), (0, 1))
            hand_over(item, 0, index)

    def take_in(item, da, db):
        ev, index = event(da, db), slot(da, db)
        wait_in(item, ev, index)
        if db == 0:
            if da == 3:
                send(item, index, 0, (1, 0), (2, 0))
            elif da == 1:
                send(item, index, 1, (3, 0), (2, 0))
            send(item, index, None, (0, 1), (da, 3))
            send(item, index, None, (0, 3), (da, 1))
        elif db == 3:
            send(item, index, 0, (0, 1), (da, 2))
        elif db == 1:
            send(item, index, 1, (0, 3), (da, 2))
        hand_over(item, ev, index)

    def own_up(start, count):
        part = pl.ds(start, count)
        for to, there in (((1, 0), (3, 0)), ((3, 0), (1, 0))):
            pltpu.make_async_remote_copy(
                src_ref=wup_hbm.at[part], dst_ref=wbuf.at[0, sp, part], send_sem=ssem.at[UP], recv_sem=rsem.at[UP, event(*there)],
                device_id=(slot(*to), x), device_id_type=MESH,
            ).start()

    with jax.named_scope("barrier"):
        pl.semaphore_wait(barrier, len(others))
    own_up(0, 16)

    with jax.named_scope("inputs"):
        for load in inputs[0:8]:
            load.wait()
    lane = lax.broadcasted_iota(jnp.int32, (64, 128), 1)
    low = lane < 64
    rowtab = rowtab_ref[...]

    def both_heads(ref):
        return jnp.concatenate([ref[...], ref[...]], axis=1)

    def rotate(v, gain, width, r, s):
        quarter = width // 4
        kind = 0 if width == 64 else 2

        def angles(which):
            across = rowtab[which * 4 + r : which * 4 + r + 1]
            if s != r:
                across = jnp.where(low[0:1], across, rowtab[which * 4 + s : which * 4 + s + 1])
            return across + coltab_ref[which]

        sq = v * v
        if width == 64:
            left = jnp.sum(jnp.where(low, sq, 0.0), axis=-1, keepdims=True)
            right = jnp.sum(jnp.where(low, 0.0, sq), axis=-1, keepdims=True)
            mean = jnp.where(low, left, right) * (1.0 / 64)
        else:
            mean = jnp.sum(sq, axis=-1, keepdims=True) * (1.0 / 128)
        u = v * lax.rsqrt(mean + EPS) * gain
        even = (lane // quarter) % 2 == 0
        turned = jnp.where(even, pltpu.roll(u, 128 - quarter, 1), pltpu.roll(u, quarter, 1))
        return u * angles(kind) + turned * angles(kind + 1)

    own = slot(0, 0)
    turned = ka_ref[...].astype(F32)
    turned = jnp.concatenate([turned[:, 0:128], turned[:, 128:256]], axis=0).T
    gain = both_heads(gka_ref)
    for r in range(2):
        block = rotate(turned[r * 64 : (r + 1) * 64], gain, 64, r, r + 2)
        kvbuf[own, r * 64 : (r + 1) * 64, :] = block.astype(BF16)
    for r in range(4):
        block = rotate(kb_ref[r * 64 : (r + 1) * 64, :].astype(F32), gkb_ref[...], 128, r, r)
        kvbuf[own, 128 + r * 64 : 192 + r * 64, :] = block.astype(BF16)
    for half in range(2):
        tokens = slice(half * 128, half * 128 + 128)
        kvbuf[own, 384 + half * 64 : 448 + half * 64, :] = va_ref[:, tokens]
        kvbuf[own, 512 + half * 128 : 640 + half * 128, :] = vb_ref[tokens, :].astype(F32).T.astype(BF16)

    take(KV, "a")
    take(KV, "b")
    loads[0].wait()
    own_up(16, 48)

    with jax.named_scope("queries"):
        for load in inputs[8:]:
            load.wait()
        gain_a = both_heads(gqa_ref)
        for g in range(2):
            lanes = slice(g * 128, g * 128 + 128)
            rows = [slice(r * 64, r * 64 + 64) for r in range(4)]
            heads = [rotate(qa_ref[rows[r], lanes].astype(F32), gain_a, 64, r, r) for r in range(4)]
            heads = jnp.concatenate(heads, axis=0).T.astype(BF16)
            for h in range(2):
                head = heads[h * 64 : h * 64 + 64]
                qa[2 * g + h, 0:64, 0:256] = head
                qa[2 * g + h, 0:64, 256:512] = jnp.zeros_like(head)
                qa[2 * g + h, 64:128, 0:256] = jnp.zeros_like(head)
                qa[2 * g + h, 64:128, 256:512] = head
            heads = [rotate(qb_ref[rows[r], lanes].astype(F32), gqb_ref[...], 128, r, r) for r in range(4)]
            qb[g] = jnp.concatenate(heads, axis=0).T.astype(BF16)
        tops[...] = jnp.full_like(tops, -1e30)
        acc_a[...] = jnp.zeros_like(acc_a)
        acc_b[...] = jnp.zeros_like(acc_b)

    scale_a = 64 ** (-0.5) * LOG2E
    scale_b = 128 ** (-0.5) * LOG2E

    def turned_values(pieces):
        values = jnp.concatenate(pieces, axis=1)
        return jnp.concatenate([values, jnp.ones((16, 512), BF16)], axis=0)

    def score(pair, target):
        keys_a = jnp.concatenate([kvbuf[s, 0:128, :] for s in pair], axis=0)
        keys_b = jnp.concatenate([kvbuf[s, 128:384, :] for s in pair], axis=0)

        def one(h):
            if h < 4:
                scores = nn_dot(keys_a, qa[h]) * scale_a
                scores = jnp.concatenate([scores[:, 0:256], scores[:, 256:512]], axis=0)
            else:
                scores = nn_dot(keys_b, qb[h - 4]) * scale_b
            target[h] = scores
            before = tops[h, 0:1, :]
            top = jnp.maximum(before, jnp.max(scores, axis=0, keepdims=True))
            tops[h, 0:1, :] = top
            tops[h, 1:2, :] = jnp.exp2(before - top)

        return one

    def gather_values(pair):
        def one(h):
            if h < 4:
                return turned_values([kvbuf[s, 384 + 64 * half : 448 + 64 * half, :] for half in range(2) for s in pair])
            return turned_values([kvbuf[s, 512 + 128 * half : 640 + 128 * half, :] for s in pair for half in range(2)])

        return one(0), one(4)

    def use(source, h, values, top, factor):
        expo = jnp.exp2(source[h] - top).astype(BF16)
        got = nn_dot(values[0] if h < 4 else values[1], expo)
        acc, index = (acc_a, h) if h < 4 else (acc_b, h - 4)
        acc[index] = acc[index] * factor + got

    def both(now, after, source, target):
        values = gather_values(now)
        scorer = None if after is None else score(after, target)
        for h in range(6):
            top, factor = tops[h, 0:1, :], tops[h, 1:2, :]
            if scorer is not None:
                scorer(h)
            use(source, h, values, top, factor)

    def my_block(t, shift):
        places = ORDER[shift::2]
        return slot(pick(t, [p[0] for p in places]), pick(t, [p[1] for p in places]))

    def partner_block(t, shift):
        places = ORDER[shift::2]
        return partner_slot(pick(t, [p[0] for p in places]), pick(t, [p[1] for p in places]))

    def ready(t, shift):
        for number in range(6):
            if PLAN.get(2 * number + shift):

                @pl.when(t == number)
                def _(number=number):
                    for what in PLAN[2 * number + shift]:
                        take(*what)

    def fetch(number, t, shift):
        theirs = partner_block(t, shift - 1)
        with jax.named_scope("pwait"):
            wait_partner(KV, number - 1, theirs)
        return my_block(t, shift + 1), theirs

    def attend(t, pair):
        with jax.named_scope("step"):
            ready(t, 2)
            middle = fetch(2 * t + 2, t, 2)
            both(pair, middle, s_odd, s_even)
            ready(t, 3)
            after = fetch(2 * t + 3, t, 3)
            both(middle, after, s_even, s_odd)
        return after

    loads[1].wait()
    with jax.named_scope("first"):
        wait_partner(KV, 0, partner)
        pair = (own, partner)
        first = score(pair, s_even)
        for h in range(6):
            first(h)
        for what in PLAN[1]:
            take(*what)
        after = (slot(*ORDER[1]), slot(*ORDER[2]))
        both(pair, after, s_even, s_odd)
    pair = lax.fori_loop(0, 6, attend, after)
    with jax.named_scope("laststep"):
        for what in PLAN[14]:
            take(*what)
        theirs = partner_slot(*ORDER[13])
        wait_partner(KV, 13, theirs)
        middle = (slot(*ORDER[15]), theirs)
        both(pair, middle, s_odd, s_even)
        for what in PLAN[15]:
            take(*what)
        after = (partner_slot(*ORDER[14]), partner_slot(*ORDER[15]))
        wait_partner(KV, 14, after[0])
        wait_partner(KV, 15, after[1])
        both(middle, after, s_even, s_odd)
        both(after, None, s_odd, None)
        for what in PLAN[16]:
            take(*what)

    for h in range(4):
        acc = acc_a[h]
        acc_a[h, 0:64, :] = acc[0:64] / acc[64:65]
    for g in range(2):
        both_rows = jnp.concatenate([acc_a[2 * g, 0:64, :], acc_a[2 * g + 1, 0:64, :]], axis=0)
        attn[:, g * 128 : (g + 1) * 128] = both_rows.T.astype(BF16)
        acc = acc_b[g]
        attn[:, 256 + g * 128 : 256 + (g + 1) * 128] = (acc[0:128] / acc[128:129]).T.astype(BF16)
    loads[2].wait()
    loads[3].wait()

    def project(j, carry):
        cols = pl.ds(pl.multiple_of(j * 512, 512), 512)
        part = jnp.dot(attn[...], wo[:, cols], preferred_element_type=F32).astype(BF16)
        for r in range(4):
            pout[r, :, cols] = part[r * 64 : (r + 1) * 64, :]
        return carry

    with jax.named_scope("project"):
        lax.fori_loop(0, 4, project, 0)

    def to_peer(forward, src, dst, send_sem, recv_sem):
        return pltpu.make_async_remote_copy(
            src_ref=src,
            dst_ref=dst,
            send_sem=send_sem,
            recv_sem=recv_sem,
            device_id=(sp, (x + (1 if forward else 3)) % 4),
            device_id_type=MESH,
        )

    class TpSum:
        def __init__(self, number, blocks, halves, received):
            self.number, self.blocks, self.halves, self.received = number, blocks, halves, received
            width = received(0).shape[1] // 2
            self.parts = (pl.ds(0, width), pl.ds(width, width))

        def copy(self, kind, way):
            near = self.blocks((x + (1, 3)[way]) % 4)
            if kind == 0:
                src, dst = self.blocks((x + 2) % 4).at[:, self.parts[way]], self.halves(way)
            else:
                part = self.parts[1 - way] if kind == 1 else self.parts[way]
                src, dst = near.at[:, part], self.received(way).at[:, part]
            return to_peer(way == 0, src, dst, xs.at[min(self.number, 1)], xr.at[self.number, min(kind, 1), way])

        def start(self):
            for kind in (0, 1):
                for way in (0, 1):
                    self.copy(kind, way).start()

        def combine(self):
            for way in (0, 1):
                self.copy(0, way).wait_recv()
                near, part = self.blocks((x + (1, 3)[way]) % 4), self.parts[way]
                near[:, part] = (near[:, part].astype(F32) + self.halves(way)[...].astype(F32)).astype(BF16)
                self.copy(2, way).start()

        def total(self):
            for way in (0, 1):
                block = self.received(way)
                to_peer(True, block, block, xs.at[0], xr.at[self.number, 1, way]).wait_recv()
            return self.blocks(x)[...].astype(F32) + self.received(0)[...].astype(F32) + self.received(1)[...].astype(F32)

    def drain_tp(ref, sem):
        three = ref.at[pl.ds(0, 3)]
        to_peer(True, three, three, sem, xr.at[0, 0, 0]).wait_send()

    proj = TpSum(0, lambda r: pout.at[r], lambda w: phalf.at[w], lambda w: rsbuf.at[w])
    proj.start()
    for what in AFTER_PROJECT:
        if what == "combine":
            with jax.named_scope("combine"):
                proj.combine()
        else:
            take(*what)
    loads[4].wait()
    with jax.named_scope("rswait"):
        total = proj.total()
    mid = (resid[...].astype(F32) + total).astype(BF16).astype(F32)
    midbuf[...] = mid
    norm = mid * lax.rsqrt(jnp.mean(mid * mid, axis=-1, keepdims=True) + EPS) * ngain_ref[...]
    nbuf[x] = norm.astype(BF16)

    halves = (pl.ds(0, 1024), pl.ds(1024, 1024))

    def rows_copy(kind, way, arriving):
        hops = (1 if kind < 2 else 2) if arriving else (0 if kind < 2 else 1)
        block = (x + 4 - hops) % 4 if way == 0 else (x + hops) % 4
        part = halves[1 - way] if kind == 1 else halves[way]
        piece = nbuf.at[block, :, part]
        return to_peer(way == 0, piece, piece, gs.at[0], gr.at[kind, way])

    for kind in (0, 1):
        for way in (0, 1):
            rows_copy(kind, way, False).start()
    for what in AFTER_SUM:
        if what == "relay":
            with jax.named_scope("relay"):
                for way in (0, 1):
                    rows_copy(0, way, True).wait_recv()
                    rows_copy(2, way, False).start()
        else:
            take(*what)
    with jax.named_scope("upwait"):
        for ev in range(16):
            wait_partner(UP, ev, partner_slot(*ORDER[ev]))
    with jax.named_scope("drainkv"):
        drain(KV)
    with jax.named_scope("rowswait"):
        for kind in (1, 2):
            for way in (0, 1):
                rows_copy(kind, way, True).wait_recv()

    def up(j, carry):
        cols = pl.ds(pl.multiple_of(j * 512, 512), 512)
        rows = nbuf[...].reshape(256, 2048)
        weights = wbuf[0, :, :, cols].reshape(2048, 512)
        part = jnp.maximum(jnp.dot(rows, weights, preferred_element_type=F32), 0.0)
        hidden[:, cols] = (part * part).astype(BF16)
        return carry

    with jax.named_scope("up"):
        lax.fori_loop(0, 2, up, 0)
    for what in AMID_UP:
        take(*what)
    with jax.named_scope("up"):
        lax.fori_loop(2, 4, up, 0)

    def chunk_sum(k):
        low_, high = CHUNKS[k]
        cols = pl.ds(low_ * 128, (high - low_) * 128)
        part = pl.ds(low_ * 64, (high - low_) * 64)
        return TpSum(k + 1, lambda r: dbuf.at[r, :, cols], lambda w: dhalf.at[w, :, part], lambda w: frecv.at[w, :, cols])

    sums = [chunk_sum(k) for k in range(len(CHUNKS))]

    last_cols = pl.ds(CHUNKS[-1][0] * 128, (CHUNKS[-1][1] - CHUNKS[-1][0]) * 128)

    def last_copy(d):
        return pltpu.make_async_remote_copy(
            src_ref=dbuf.at[(x + d) % 4, :, last_cols], dst_ref=lastbuf.at[d - 1], send_sem=xs.at[1], recv_sem=lr.at[d - 1],
            device_id=(sp, (x + d) % 4), device_id_type=MESH,
        )

    def last_total():
        total = dbuf[x, :, last_cols].astype(F32)
        for d in (1, 3, 2):
            last_copy(d).wait_recv()
            total = total + lastbuf[d - 1].astype(F32)
        return total

    def collect(k):
        total = last_total() if k == len(CHUNKS) - 1 else sums[k].total()
        places = ORDER[slice(*CHUNKS[k])]
        blocks = [slot(*place) for place in places] + [partner_slot(*place) for place in places]
        for b, block in enumerate(blocks):
            piece = total[:, (b // 2) * 128 : (b // 2) * 128 + 128]
            if b % 2 == 1:
                piece = pltpu.roll(piece, 64, 1)
            stage[block] = piece

    def down(k):
        first_, last_ = CHUNKS[k]
        places = ORDER[first_:last_]
        with jax.named_scope("dwait"):
            for r in range(first_, last_):
                wait_partner(DOWN, r, partner_slot(*ORDER[r]))
        blocks = [slot(*place) for place in places] + [partner_slot(*place) for place in places]
        part = nt_dot(hidden[...], jnp.concatenate([wbuf[1, b] for b in blocks], axis=0)).astype(BF16)
        for r in range(4):
            dbuf[r, :, first_ * 128 : last_ * 128] = part[r * 64 : (r + 1) * 64, :]
        if k == len(CHUNKS) - 1:
            for d in (2, 1, 3):
                last_copy(d).start()
        else:
            sums[k].start()

    for what in TAIL:
        if isinstance(what, tuple):
            take(*what)
        else:
            with jax.named_scope(what):
                kind, k = what[:-1], int(what[-1])
                if kind == "down":
                    down(k)
                elif kind == "combine":
                    sums[k].combine()
                else:
                    collect(k)
    drain(UP)
    drain(DOWN)
    drain_tp(pout, xs.at[0])
    drain_tp(nbuf, gs.at[0])
    with jax.named_scope("assemble"):
        for pos in range(16):
            both_halves = jnp.where(low, stage[2 * pos], pltpu.roll(stage[2 * pos + 1], 64, 1))
            cols = slice(pos * 128, pos * 128 + 128)
            out_ref[:, cols] = (midbuf[:, cols] + both_halves).astype(BF16)

    with jax.named_scope("draintp"):
        drain_tp(dbuf, xs.at[1])


def local(
    resid, query_a, key_a, value_a, query_b, key_b, value_b, gain_qa, gain_ka, gain_qb, gain_kb,
    w_out_a, w_out_b, norm_gain, w_up, w_down,
):
    rowtab, coltab = build_tables()
    vmem = pl.BlockSpec(memory_space=pltpu.VMEM)
    anywhere = pl.BlockSpec(memory_space=pl.ANY)
    dma = pltpu.SemaphoreType.DMA
    return pl.pallas_call(
        kernel,
        out_shape=pltpu.VMEM((64, 2048), BF16),
        in_specs=[anywhere] * 18,
        out_specs=vmem,
        scratch_shapes=[
            pltpu.VMEM((64, 256), BF16),
            pltpu.VMEM((64, 256), BF16),
            pltpu.VMEM((256, 128), BF16),
            pltpu.VMEM((256, 128), BF16),
            pltpu.VMEM((1, 64), F32),
            pltpu.VMEM((1, 128), F32),
            pltpu.VMEM((16, 128), F32),
            pltpu.VMEM((4, 64, 128), F32),
            pltpu.VMEM((256, 256), BF16),
            pltpu.VMEM((256, 256), BF16),
            pltpu.VMEM((1, 64), F32),
            pltpu.VMEM((1, 128), F32),
            pltpu.VMEM((1, 2048), F32),
            pltpu.VMEM((32, 768, 128), BF16),
            pltpu.VMEM((2, 32, 64, 2048), BF16),
            pltpu.VMEM((512, 2048), BF16),
            pltpu.VMEM((64, 2048), BF16),
            pltpu.VMEM((4, 128, 512), BF16),
            pltpu.VMEM((2, 128, 256), BF16),
            pltpu.VMEM((6, 512, 256), F32),
            pltpu.VMEM((6, 512, 256), F32),
            pltpu.VMEM((6, 8, 256), F32),
            pltpu.VMEM((4, 80, 256), F32),
            pltpu.VMEM((2, 144, 256), F32),
            pltpu.VMEM((256, 512), BF16),
            pltpu.VMEM((4, 64, 2048), BF16),
            pltpu.VMEM((2, 64, 1024), BF16),
            pltpu.VMEM((2, 64, 2048), BF16),
            pltpu.VMEM((4, 64, 2048), BF16),
            pltpu.VMEM((256, 2048), BF16),
            pltpu.VMEM((4, 64, 2048), BF16),
            pltpu.VMEM((2, 64, 1024), BF16),
            pltpu.VMEM((2, 64, 2048), BF16),
            pltpu.VMEM((32, 64, 128), F32),
            pltpu.VMEM((64, 2048), F32),
            pltpu.VMEM((3, 64, 256), BF16),
            dma((18,)),
            dma((3,)),
            dma((3, 16)),
            dma((3, 16)),
            dma((2,)),
            dma((5, 2, 2)),
            dma((1,)),
            dma((3, 2)),
            dma((3,)),
        ],
        compiler_params=pltpu.CompilerParams(
            collective_id=0, has_side_effects=True, vmem_limit_bytes=58 * 1024 * 1024
        ),
    )(
        key_a.T, value_a.T, key_b, value_b, gain_ka.reshape(1, -1), gain_kb.reshape(1, -1),
        jnp.asarray(rowtab), jnp.asarray(coltab),
        query_a, query_b, gain_qa.reshape(1, -1), gain_qb.reshape(1, -1), norm_gain.reshape(1, -1),
        resid, w_out_a, w_out_b, w_up, w_down.T,
    )


def solution(mesh):
    return jax.shard_map(
        local,
        mesh=mesh,
        in_specs=(
            P(("sp", "tp"), None),
            P("sp", "tp"),
            P("sp", "tp"),
            P("sp", "tp"),
            P("sp", "tp"),
            P("sp", "tp"),
            P("sp", "tp"),
            P(),
            P(),
            P(),
            P(),
            P("tp", None),
            P("tp", None),
            P(),
            P("sp", "tp"),
            P("tp", "sp"),
        ),
        out_specs=P(("sp", "tp"), None),
        check_vma=False,
    )
```
